32 devices in a mesh: ep: 8 (over z, x), tp: 4 (over y, core).
Axes of the slice: x: 2, y: 2, z: 4, core: 2. Of those that a mesh axis runs over, the one named last changes fastest.
Arguments:
- tokens: bfloat16 [4608, 2048], P(('ep', 'tp')), may hold values from -6 to 6
- norm_gain: float32 [2048], replicated, may hold values from 0.1 to 1.9
- expert_ids: int32 [4608, 8], P(('ep', 'tp')), may hold values from 0 to 15, all different within a row; in each aligned block of 144 rows (0 to 143, 144 to 287, ...) at most 144 rows name the same one
- route_weights: float32 [4608, 8], P(('ep', 'tp')), may hold values from 0.3 to 1
- expert_gate: bfloat16 [16, 512, 2048], P('ep', 'tp'), may hold values from -0.125 to 0.125
- expert_up: bfloat16 [16, 512, 2048], P('ep', 'tp'), may hold values from -0.125 to 0.125
- expert_down: bfloat16 [16, 512, 2048], P('ep', 'tp'), may hold values from -0.25 to 0.25
- shared_gate: bfloat16 [512, 2048], P('tp'), may hold values from -0.125 to 0.125
- shared_up: bfloat16 [512, 2048], P('tp'), may hold values from -0.125 to 0.125
- shared_down: bfloat16 [512, 2048], P('tp'), may hold values from -0.25 to 0.25
- side_in: bfloat16 [2048, 1024], P('ep'), may hold values from -0.125 to 0.125
- side_out: bfloat16 [2048, 1024], P('ep'), may hold values from -0.1875 to 0.1875
- side_gate: bfloat16 [2048], replicated, may hold values from -0.125 to 0.125
Outputs:
- mixed: bfloat16 [4608, 2048], P(('ep', 'tp'))
The draws below stay inside these ranges and needn't reach their ends.
Inputs may be any that keep to these rules, and one draw needn't show every extreme that they name: `expert_ids`: each row names 8 different experts of 0 to 15; within the rows of one device (aligned blocks of 144 rows) no expert is named more than 144 times, and in some of those blocks some expert is named exactly 144 times.
All inputs are finite; a program needn't handle non-finite values.
Results may differ from the reference program's by a relative error of at most 0.0068.
Values may be sent and summed in bfloat16 or wider, within the bound.
A program may use at most 320 MiB of HBM per device.

```python
import math
import jax
import jax.numpy as jnp
import numpy as np
from jax import lax

D = 2048
FF = 512
SIDE = 1024
TOP = 8
TOK_DEV = 144
EXPERTS = 16
CAP = 144
TOKENS = 4608


def levels(stream_key, extent, pieces, smallest, largest):
    level = 1.0
    for dim, blocks in pieces:
        steps = jax.random.uniform(jax.random.fold_in(jax.random.fold_in(stream_key, 6), dim), (blocks,), jnp.float32, smallest / len(pieces), largest / len(pieces))
        level = level * jnp.repeat(jnp.exp(steps), extent[dim] // blocks).reshape((-1,) + (1,) * (len(extent) - 1 - dim))
    return level


def shared_out(rng, own, number, rows, number_of, top, bound, skew):
    ranking = jax.random.permutation(rng, number_of)
    heavy_load, common = portions_of(number_of, rows * top, bound, skew, True), portions_of(number_of, rows * top, bound, skew, False)
    places = jnp.arange(number_of)

    def named(lengths, rotation):
        used = int((lengths > 0).sum())
        fixed = max(1, used // 4)
        shifted = fixed + (places - fixed + rotation * (used - fixed)) % max(1, number_of - fixed)
        return jnp.zeros((number_of,), jnp.int32).at[ranking[jnp.where(places < fixed, places, shifted)]].set(jnp.asarray(lengths, jnp.int32))

    lengths = jnp.where(number % 4 == 0, named(heavy_load, number // 4), named(common, number - number // 4 - 1))
    mixed = jax.random.permutation(jax.random.fold_in(own, 3), number_of)
    source_of, receiver = mixed[0:number_of // 2 * 2:2], mixed[1:number_of // 2 * 2:2]
    slack = jnp.minimum(lengths[source_of] - 1, bound - lengths[receiver]) // 2
    slack = jnp.where((source_of == ranking[0]) | (receiver == ranking[0]) | (lengths[receiver] == 0), 0, jnp.maximum(slack, 0))
    shifted = jax.random.randint(jax.random.fold_in(own, 4), (number_of // 2,), 0, 1 << 20) % (slack + 1)
    lengths = lengths.at[source_of].add(-shifted).at[receiver].add(shifted)
    items = jnp.searchsorted(jnp.cumsum(lengths), jnp.arange(rows * top), side="right").astype(jnp.int32)
    listing = items.reshape(top, rows).T
    listing = listing[jax.random.permutation(jax.random.fold_in(own, 1), rows)]
    rotation = jax.random.randint(jax.random.fold_in(own, 2), (rows, 1), 0, top)
    return jnp.take_along_axis(listing, (jnp.arange(top)[None, :] + rotation) % top, axis=1)


def portions_of(amount, total, reach, slope, full):
    loads = [(1 << 20) // math.isqrt(rank ** slope) + 1 for rank in range(1, amount + 1)]
    largest = reach if full else min(reach, max(-(-total // amount), total * loads[0] // sum(loads)))
    least = 1 if total - largest >= amount - 1 else 0
    holding, spare = [largest] + [least] * (amount - 1), total - largest - least * (amount - 1)
    while spare > 0:
        free = [i for i in range(1, amount) if holding[i] < largest] or [i for i in range(1, amount) if holding[i] < reach]
        pool, left = sum([loads[i] for i in free]), spare
        for i in free:
            addition = min(reach - holding[i], max(1, left * loads[i] // pool), spare)
            holding[i] = holding[i] + addition
            spare = spare - addition
    return np.array(holding)


def centred(key, dims, scale, reach, split=(), kind=jnp.bfloat16):
    gain = levels(key, dims, split, -0.22, 0.18) if split else 1.0
    array = jax.random.normal(key, dims, jnp.float32) * scale * gain
    return jnp.minimum(jnp.maximum(array, -reach), reach).astype(kind)


def setup_inputs(seed: int = 0) -> dict:
    arg_keys = jax.random.split(jax.random.key(seed), 14)
    tokens = centred(arg_keys[0], (TOKENS, D), 1.0, 6.0, ((0, 32),))
    norm_gain = jnp.clip(1.0 + 0.18 * jax.random.normal(arg_keys[1], (D,), jnp.float32), 0.1, 1.9)
    expert_ids_keys = jax.random.split(jax.random.fold_in(arg_keys[2], 1), TOKENS // TOK_DEV)
    expert_ids_turns = jax.random.permutation(jax.random.fold_in(arg_keys[2], 3), TOKENS // TOK_DEV)
    expert_ids = jax.vmap(lambda own, number: shared_out(jax.random.fold_in(arg_keys[2], 2), own, number, TOK_DEV, EXPERTS, TOP, CAP, 2))(expert_ids_keys, expert_ids_turns).reshape((TOKENS, TOP))
    route_weights = jnp.clip(0.3 + 0.7 * jax.random.uniform(arg_keys[3], (TOKENS, TOP), jnp.float32) ** levels(arg_keys[3], (TOKENS, TOP), ((0, 32),), -0.2, 0.2), 0.3, 1.0)
    expert_gate = centred(arg_keys[4], (EXPERTS, FF, D), D ** -0.5, 0.125, ((0, 8), (1, 4)))
    expert_up = centred(arg_keys[5], (EXPERTS, FF, D), D ** -0.5, 0.125, ((0, 8), (1, 4)))
    expert_down = centred(arg_keys[6], (EXPERTS, FF, D), FF ** -0.5, 0.25, ((0, 8), (1, 4)))
    shared_gate = centred(arg_keys[7], (FF, D), D ** -0.5, 0.125, ((0, 4),))
    shared_up = centred(arg_keys[8], (FF, D), D ** -0.5, 0.125, ((0, 4),))
    shared_down = centred(arg_keys[9], (FF, D), FF ** -0.5, 0.25, ((0, 4),))
    side_in = centred(arg_keys[10], (D, SIDE), D ** -0.5, 0.125, ((0, 8),))
    side_out = centred(arg_keys[11], (D, SIDE), SIDE ** -0.5, 0.1875, ((0, 8),))
    side_gate = centred(arg_keys[12], (D,), D ** -0.5, 0.125)
    return dict(tokens=tokens, norm_gain=norm_gain, expert_ids=expert_ids, route_weights=route_weights, expert_gate=expert_gate, expert_up=expert_up, expert_down=expert_down, shared_gate=shared_gate, shared_up=shared_up, shared_down=shared_down, side_in=side_in, side_out=side_out, side_gate=side_gate)


norm_eps = 1.0
row_block = 512

def normalize(tokens, norm_gain):
    values = tokens.astype(jnp.float32)
    scale_inv = lax.rsqrt(lax.optimization_barrier(jnp.mean(values * values, axis=-1, keepdims=True)) + norm_eps)
    return (values * scale_inv * norm_gain).astype(jnp.bfloat16)

def swiglu(gate_part, up_part):
    return (jax.nn.silu(gate_part) * up_part).astype(jnp.bfloat16)

def reference(tokens, norm_gain, expert_ids, route_weights, expert_gate, expert_up, expert_down, shared_gate, shared_up, shared_down, side_in, side_out, side_gate):
    normed = normalize(tokens, norm_gain)
    pair_count = TOKENS * TOP
    flat_ids = expert_ids.reshape(pair_count).astype(jnp.int32)
    flat_tokens = (jnp.arange(pair_count, dtype=jnp.int32) // TOP).astype(jnp.int32)
    flat_weights = route_weights.reshape(pair_count)
    order = jnp.argsort(flat_ids, stable=True)
    sorted_ids = flat_ids[order]
    counts = jnp.bincount(flat_ids, length=EXPERTS).astype(jnp.int32)
    starts = (jnp.cumsum(counts) - counts).astype(jnp.int32)
    padded = ((counts + row_block - 1) // row_block * row_block).astype(jnp.int32)
    ends = jnp.cumsum(padded).astype(jnp.int32)
    begins = (ends - padded).astype(jnp.int32)
    target = (begins[sorted_ids] + jnp.arange(pair_count, dtype=jnp.int32) - starts[sorted_ids]).astype(jnp.int32)
    block_count = (pair_count + EXPERTS * (row_block - 1)) // row_block + 1
    slots_all = block_count * row_block
    token_slots = jnp.full((slots_all,), TOKENS, jnp.int32).at[target].set(flat_tokens[order])
    weight_slots = jnp.zeros((slots_all,), jnp.float32).at[target].set(flat_weights[order])
    block_starts = (jnp.arange(block_count, dtype=jnp.int32) * row_block).astype(jnp.int32)
    block_expert = jnp.minimum(jnp.searchsorted(ends, block_starts, side='right'), EXPERTS - 1).astype(jnp.int32)
    extended = jnp.concatenate([normed, jnp.zeros((1, D), normed.dtype)], axis=0)

    def block_step(running, inputs):
        slot_tokens, slot_weights, expert = inputs
        chosen = extended[slot_tokens]
        gate_part = jnp.dot(chosen, expert_gate[expert].T, preferred_element_type=jnp.float32)
        up_part = jnp.dot(chosen, expert_up[expert].T, preferred_element_type=jnp.float32)
        hidden = swiglu(gate_part, up_part)
        output = jnp.dot(hidden, expert_down[expert], preferred_element_type=jnp.float32).astype(jnp.bfloat16)
        output = lax.optimization_barrier(output).astype(jnp.float32)
        return (running.at[slot_tokens].add(output * slot_weights[:, None]), None)
    running = jnp.zeros((TOKENS + 1, D), jnp.float32)
    running, unused = lax.scan(block_step, running, (token_slots.reshape(block_count, row_block), weight_slots.reshape(block_count, row_block), block_expert))
    routed = running[:TOKENS]
    shared_hidden = swiglu(jnp.dot(normed, shared_gate.T, preferred_element_type=jnp.float32), jnp.dot(normed, shared_up.T, preferred_element_type=jnp.float32))
    shared = jnp.dot(shared_hidden, shared_down, preferred_element_type=jnp.float32)
    side_hidden = jax.nn.silu(jnp.dot(normed, side_in, preferred_element_type=jnp.float32)).astype(jnp.bfloat16)
    side_value = jnp.dot(side_hidden, side_out.T, preferred_element_type=jnp.float32)
    opening = jax.nn.sigmoid(jnp.dot(normed, side_gate, preferred_element_type=jnp.float32))
    return (routed + shared + opening[:, None] * side_value).astype(jnp.bfloat16)
```

```python
import functools

import jax
import jax.numpy as jnp
from jax import lax
from jax.experimental import pallas as pl
from jax.experimental.pallas import tpu as pltpu
from jax.sharding import PartitionSpec as P

norm_eps = 1.0
MESH = pl.DeviceIdType.MESH
NT = (((1,), (1,)), ((), ()))


def silu(v):
    return v / (1.0 + jnp.exp(-v))


def when(conds, act):
    conds = [cond() for cond in conds]
    if any(cond is False for cond in conds):
        return
    conds = [cond for cond in conds if cond is not True]
    if not conds:
        act()
        return
    both = conds[0]
    for cond in conds[1:]:
        both = jnp.logical_and(both, cond)
    pl.when(both)(act)


def kernel(
    dims,
    tokens_ref, gain_ref, ids_ref, route_ref, side_gate_ref,
    gate_ref, up_ref, down_ref, s_gate_ref, s_up_ref, s_down_ref, side_in_ref, side_out_ref,
    out_ref,
    tok, wall, side, hidden, side_hid, acc, xs, xr, sent, got, hgot, saux, sc, scol,
    tok_send, tok_recv, hyb_send, w_send, w_recv, side_send, side_recv, swap_send, swap_recv,
    local_sem, aux_send, aux_recv, x_send, x_recv, r_send, l_send, z_recv, h_send, h_recv,
):
    nz, nx, ny, nc, local_experts, pieces, extra, chunks, ahead = dims
    n_ep, n_tp = nz * nx, ny * nc
    me, tp = lax.axis_index("ep"), lax.axis_index("tp")
    z, x = me // nx, me % nx
    y, c = tp // nc, tp % nc
    rows, width = tokens_ref.shape
    routed = gate_ref.shape[0]
    pr = routed // pieces
    per_expert = pieces // local_experts
    piece_units, shared_units = n_tp * pr, n_tp * extra
    side_rows, side_cols = side.shape[1:]
    piece = width // chunks
    half_w = width // 2
    down_at = 2 * (routed + extra)
    tile = 2 * rows
    hyb = nx == 2 and nz == 4
    tiles = n_ep // 2

    near = [
        sorted(range(nz), key=lambda b: (abs(b - zz), -b if 2 * zz < nz else b))
        for zz in range(nz)
    ]
    place_of = [[near[zz].index(b) for b in range(nz)] for zz in range(nz)]

    def by_z(values):
        out = values[0]
        if all(v == out for v in values):
            return out
        for zz in range(1, nz):
            out = jnp.where(z == zz, values[zz], out)
        return out

    def flag(values):
        values = [bool(v) for v in values]
        if all(values) or not any(values):
            return values[0]
        return by_z([int(v) for v in values]) == 1

    ends = lambda: flag([zz in (0, nz - 1) for zz in range(nz)])
    inner = lambda: flag([zz not in (0, nz - 1) for zz in range(nz)])
    twin = z + 1 - 2 * (z % 2)

    def slot(j, k):
        return k // 2 * (2 * nx) + 2 * j + k % 2

    def cols(q):
        return pl.ds(q * piece, piece)

    barrier = pltpu.get_barrier_semaphore()
    for j in range(1, n_ep):
        pl.semaphore_signal(barrier, inc=1, device_id=((me + j) % n_ep, tp), device_id_type=MESH)
    for j in range(1, n_tp):
        pl.semaphore_signal(barrier, inc=1, device_id=(me, (tp + j) % n_tp), device_id_type=MESH)


    def slot_rows(s):
        return pl.ds(s * rows if isinstance(s, int) else pl.multiple_of(s * rows, 16), rows)

    def tok_copy(from_slot, to_slot, h, target, send):
        part = pl.ds(h * half_w, half_w)
        return pltpu.make_async_remote_copy(
            src_ref=tok.at[slot_rows(from_slot), part],
            dst_ref=tok.at[slot_rows(to_slot), part],
            send_sem=send, recv_sem=tok_recv.at[to_slot, h],
            device_id=target, device_id_type=MESH,
        )

    def tok_wait(s, h):
        tok_copy(s, s, h, (me, tp), tok_send.at[0, 0, 0]).wait_recv()

    def along(k, h, d):
        to = by_z([
            place_of[zz + d][near[zz][k]] if 0 <= zz + d < nz else 0 for zz in range(nz)
        ])
        return tok_copy(
            slot(0, k), slot(0, to), h, (me + d * nx, tp), tok_send.at[k, (1 - d) // 2, h]
        )

    def across(k, h, j):
        return tok_copy(
            slot(0, k), slot(nx - j, k), h, (z * nx + (x + j) % nx, tp), tok_send.at[k, 1 + j, h]
        )

    def onward(k, to, h):
        return tok_copy(
            slot(1, k), slot(1, to), h, (me + (twin - z) * nx, tp), hyb_send.at[h]
        )

    def crosses(k, h):
        if hyb and k == nz - 1 and h == 1:
            return inner
        if hyb and k == nz - 2:
            return ends
        return lambda: True

    log = []

    def launch(conds, copy):
        log.append((conds, copy))
        when(conds, lambda: copy().start())

    def send_block(conds, k, h):
        bind = functools.partial
        for d in (1, -1):
            goes = [
                0 <= zz + d < nz and (near[zz][k] - zz) * d <= 0 for zz in range(nz)
            ]
            launch(conds + [lambda goes=goes: flag(goes)], bind(along, k, h, d))
        for j in range(1, nx):
            launch(conds + [crosses(k, h)], bind(across, k, h, j))

    def stage(step, h):
        for k in range(1, nz):
            here = [abs(near[zz][k] - zz) == step for zz in range(nz)]
            if any(here):
                cond = lambda here=here: flag(here)
                when([cond], lambda: tok_wait(slot(0, k), h))
                send_block([cond], k, h)
        if hyb and step == 1:
            tok_wait(slot(1, 0), h)
            launch([ends], functools.partial(onward, 0, nz - 2, h))
        if hyb and step == nz - 1 and h == 1:
            when([inner], lambda: tok_wait(slot(1, nz - 1), 1))
            launch([inner], functools.partial(onward, nz - 1, nz - 1, 1))

    def cross_wait(half):
        for j in range(1, nx):
            for k in (2 * half, 2 * half + 1):
                for h in range(2):
                    if hyb and k == 0:
                        continue
                    conds = [ends] if hyb and k == nz - 1 and h == 1 else []
                    when(conds, lambda: tok_wait(slot(j, k), h))


    shared_at = pl.ds(0, extra)
    if s_gate_ref.shape[0] > extra:
        shared_at = pl.ds(pl.multiple_of(me * extra, extra), extra)

    def w_parts(k):
        slab = wall.at[tp]
        if k < pieces:
            at, r0 = pl.ds(k * pr, pr), 2 * extra + 2 * k * pr
            parts = [
                (gate_ref.at[at], slab.at[pl.ds(r0, pr)]),
                (up_ref.at[at], slab.at[pl.ds(r0 + pr, pr)]),
            ]
            if k == 0:
                parts += [
                    (s_gate_ref.at[shared_at], slab.at[pl.ds(0, extra)]),
                    (s_up_ref.at[shared_at], slab.at[pl.ds(extra, extra)]),
                ]
            return parts
        q = cols(k - pieces)
        return [
            (down_ref.at[:, q], slab.at[pl.ds(down_at, routed), q]),
            (s_down_ref.at[shared_at, q], slab.at[pl.ds(down_at + routed, extra), q]),
        ]

    def w_place(k, owner):
        if k == 0:
            return wall.at[owner, pl.ds(0, 2 * (extra + pr))]
        if k < pieces:
            return wall.at[owner, pl.ds(2 * (extra + k * pr), 2 * pr)]
        return wall.at[owner, pl.ds(down_at, routed + extra), cols(k - pieces)]

    def w_copy(k, by, way, refs=None):
        if way < 2:
            target = (me, tp + nc if way == 0 else tp - nc)
        else:
            target = (me, y * nc + (c + way - 1) % nc)
        owner = by * nc + c
        if refs is None:
            refs = (wall.at[owner],) * 2 if k is None else (w_place(k, owner),) * 2
        return pltpu.make_async_remote_copy(
            src_ref=refs[0], dst_ref=refs[1], send_sem=w_send.at[by, way],
            recv_sem=w_recv.at[0 if k is None else k, owner],
            device_id=target, device_id_type=MESH,
        )

    def w_wait(k, owner):
        pltpu.make_async_remote_copy(
            src_ref=w_place(k, owner), dst_ref=w_place(k, owner), send_sem=w_send.at[0, 0],
            recv_sem=w_recv.at[k, owner], device_id=(me, tp), device_id_type=MESH,
        ).wait_recv()

    def each_own(copy_of, act):
        pl.when(y < ny - 1)(lambda: act(copy_of(0)))
        pl.when(y > 0)(lambda: act(copy_of(1)))
        for way in range(2, 1 + nc):
            act(copy_of(way))

    def each_forward(copy_of, step, act, arrive):
        @pl.when(y >= step)
        def _():
            b = y - step
            arrive(b)
            pl.when(y < ny - 1)(lambda: act(copy_of(b, 0)))
            for way in range(2, 1 + nc):
                act(copy_of(b, way))

        @pl.when(y + step <= ny - 1)
        def _():
            b = y + step
            arrive(b)
            pl.when(y > 0)(lambda: act(copy_of(b, 1)))
            for way in range(2, 1 + nc):
                act(copy_of(b, way))

    start = lambda copy: copy.start()
    finish = lambda copy: copy.wait_send()

    def w_gathered(k):
        for step in range(1, ny):
            each_forward(
                lambda b, way: w_copy(k, b, way), step, start, lambda b: w_wait(k, b * nc + c)
            )

    def w_across(k):
        for j in range(1, nc):
            for by in range(ny):
                w_wait(k, by * nc + (c + j) % nc)


    def side_source(ref, to):
        if len(ref.shape) == 3:
            return ref.at[to]
        return ref.at[:, pl.ds(pl.multiple_of(to * side_cols, side_cols), side_cols)]

    def side_copy(j, p):
        to = (me + j) % n_ep
        return pltpu.make_async_remote_copy(
            src_ref=side_source((side_in_ref, side_out_ref)[p], to),
            dst_ref=side.at[p * n_ep + me],
            send_sem=side_send, recv_sem=side_recv, device_id=(to, tp), device_id_type=MESH,
        )

    def side_all():
        whole = side.at[pl.ds(0, n_ep - 1)]
        return pltpu.make_async_remote_copy(
            src_ref=whole, dst_ref=whole, send_sem=side_send, recv_sem=side_recv,
            device_id=(me, tp), device_id_type=MESH,
        )

    def side_own(p):
        return pltpu.make_async_copy(
            side_source((side_in_ref, side_out_ref)[p], me), side.at[p * n_ep + me],
            local_sem.at[1],
        )

    def swap_copy(half):
        part = side.at[pl.ds(half * n_ep, n_ep)]
        return pltpu.make_async_remote_copy(
            src_ref=part, dst_ref=part, send_sem=swap_send, recv_sem=swap_recv,
            device_id=(me, y * nc + 1 - c), device_id_type=MESH,
        )


    def aux_copy(k, j):
        to = by_z([near[zz][k] for zz in range(nz)]) * nx + (x + j) % nx
        k_there = by_z([place_of[near[zz][k]][zz] for zz in range(nz)])
        return pltpu.make_async_remote_copy(
            src_ref=saux.at[to], dst_ref=sc.at[slot((nx - j) % nx, k_there)],
            send_sem=aux_send, recv_sem=aux_recv, device_id=(to, tp), device_id_type=MESH,
        )

    def aux_all():
        return pltpu.make_async_remote_copy(
            src_ref=saux.at[pl.ds(0, n_ep - 1)], dst_ref=sc.at[pl.ds(0, n_ep - 1)],
            send_sem=aux_send, recv_sem=aux_recv, device_id=(me, tp), device_id_type=MESH,
        )

    for k in range(pieces + chunks):
        for part in w_parts(k):
            pltpu.make_async_copy(*part, local_sem.at[0]).start()
    for p in range(nc):
        pl.when(c == p)(lambda: side_own(p).start())

    values = tokens_ref[...].astype(jnp.float32)
    scale_inv = lax.rsqrt(jnp.mean(values * values, axis=-1, keepdims=True) + norm_eps)
    normed = (values * scale_inv * gain_ref[...]).astype(jnp.bfloat16)
    tok[slot_rows(0), :] = normed

    pl.semaphore_wait(barrier, n_ep + n_tp - 2)
    for h in range(2):
        send_block([], 0, h)
    for k in range(pieces + chunks):
        for refs in w_parts(k):
            each_own(lambda way: w_copy(k, y, way, refs), start)

    side_vector = side_gate_ref[...].astype(jnp.float32)
    lanes = side_vector.shape[1]
    side_vector = jnp.concatenate(
        [jnp.broadcast_to(side_vector[i : i + 1], (8, lanes)) for i in range(width // lanes)],
        axis=1,
    ).astype(jnp.bfloat16)
    opening = lax.dot_general(side_vector, normed, NT, preferred_element_type=jnp.float32)
    opening = 1.0 / (1.0 + jnp.exp(-opening))
    ids, route = ids_ref[...], route_ref[...]
    row = lax.broadcasted_iota(jnp.int32, (8, rows), 0)
    for to in range(n_ep):
        block = jnp.where(row == local_experts, opening, 0.0)
        for e in range(local_experts):
            hit = jnp.where(ids == to * local_experts + e, route, 0.0)
            block = jnp.where(row == e, jnp.sum(hit, axis=0, keepdims=True), block)
        gap = sc.shape[2] - rows
        saux[to] = jnp.concatenate([block, jnp.zeros((8, gap), jnp.float32)], axis=1)
    sc[0] = saux[me]
    for k in range(nz):
        for j in range(nx):
            if k or j:
                aux_copy(k, j).start()


    def tile_rows(t):
        return pl.ds(pl.multiple_of(t * tile, 16), tile)

    def column(at, n):
        picked = scol[at, :]
        lane = lax.broadcasted_iota(jnp.int32, picked.shape, 1)
        return jnp.sum(jnp.where(lane == n, picked, 0.0), axis=1, keepdims=True)

    def nt(a, b):
        return lax.dot_general(a, b, NT, preferred_element_type=jnp.float32)

    def unit(t, p):
        at = tile_rows(t)
        r0 = 2 * extra + p * (2 * pr)
        if not isinstance(p, int):
            r0 = pl.multiple_of(r0, 16)
        a = tok[at, :]
        gate = wall[:, pl.ds(r0, pr), :].reshape(piece_units, width)
        up = wall[:, pl.ds(r0 + pr, pr), :].reshape(piece_units, width)
        gated = silu(nt(a, gate)) * nt(a, up) * column(at, p // per_expert)
        to = p * piece_units if isinstance(p, int) else pl.multiple_of(p * piece_units, 128)
        hidden[at, pl.ds(to, piece_units)] = gated.astype(jnp.bfloat16)

    def units(t0, t1, p0, p1):
        n = p1 - p0
        if (t1 - t0) * n > 0:
            def step(i, carry):
                unit(t0 + i // n, p0 + i % n)
                return carry

            lax.fori_loop(0, (t1 - t0) * n, step, 0)

    def extras(t0, t1):
        def step(t, carry):
            at = tile_rows(t)
            a = tok[at, :]
            both = jnp.concatenate([
                wall[:, :extra, :].reshape(shared_units, width),
                wall[:, extra : 2 * extra, :].reshape(shared_units, width),
            ], axis=0)
            both = nt(a, both)
            gated = silu(both[:, :shared_units]) * both[:, shared_units:]
            hidden[at, pieces * piece_units :] = gated.astype(jnp.bfloat16)
            side_part = jnp.dot(
                a, side[:n_ep].reshape(width, side_cols), preferred_element_type=jnp.float32
            )
            side_hid[at] = (silu(side_part) * column(at, local_experts)).astype(jnp.bfloat16)
            return carry

        lax.fori_loop(t0, t1, step, 0)

    def arrive(k):
        w_gathered(k)
        w_across(k)

    for h in range(2):
        stage(1, h)
    for p in range(nc):
        def side_go(p=p):
            for j in range(1, n_ep):
                side_copy(j, p).start()

        pl.when(c == p)(side_go)
    pltpu.make_async_copy(wall.at[tp], wall.at[tp], local_sem.at[0]).wait()
    aux_all().wait_recv()
    for s in range(n_ep):
        scol[slot_rows(s), :] = sc[s].T[:rows]
    arrive(0)
    units(0, 1, 0, 1)
    stage(2, 0)
    arrive(1)
    units(0, 1, 1, 2)
    stage(2, 1)
    cross_wait(0)
    units(1, nx, 0, 2)
    for s in range(3, nz):
        stage(s, 0)
    for p in range(2, pieces - 1):
        arrive(p)
    units(0, nx, 2, pieces - 1)
    for s in range(3, nz):
        stage(s, 1)
    for p in range(nc):
        pl.when(c == p)(lambda: side_own(p).wait())
    side_all().wait_recv()
    swap_copy(c).start()
    units(nx, nx + 1, 0, pieces - 1)
    swap_copy(1 - c).wait_recv()
    extras(0, nx + 1)
    for half in range(1, nz // 2):
        cross_wait(half)
    units(nx + 1, tiles, 0, pieces - 1)
    arrive(pieces - 1)
    units(0, tiles, pieces - 1, pieces)
    extras(nx + 1, tiles)


    def x_index(j, k, q):
        return ((j - 1) * nz + k) * chunks + q

    def x_copy(q, j, k):
        i = x_index(j, k, q)
        return pltpu.make_async_remote_copy(
            src_ref=xs.at[i], dst_ref=xr.at[i], send_sem=x_send, recv_sem=x_recv.at[i],
            device_id=(z * nx + (x + j) % nx, tp), device_id_type=MESH,
        )

    def x_total(n):
        return pltpu.make_async_remote_copy(
            src_ref=xs.at[pl.ds(0, n)], dst_ref=xr.at[pl.ds(0, n)], send_sem=x_send,
            recv_sem=x_recv.at[0], device_id=(me, tp), device_id_type=MESH,
        )

    def h_copy(k, q):
        return pltpu.make_async_remote_copy(
            src_ref=xs.at[x_index(1, k, q)], dst_ref=hgot.at[q], send_sem=h_send,
            recv_sem=h_recv.at[q], device_id=(me + (twin - z) * nx, tp), device_id_type=MESH,
        )

    def h_total(n):
        return pltpu.make_async_remote_copy(
            src_ref=xs.at[pl.ds(0, n)], dst_ref=hgot.at[pl.ds(0, n)], send_sem=h_send,
            recv_sem=h_recv.at[0], device_id=(me, tp), device_id_type=MESH,
        )

    def z_copy(q, dz, right):
        return pltpu.make_async_remote_copy(
            src_ref=sent.at[dz * chunks + q], dst_ref=got.at[(dz + right) * chunks + q],
            send_sem=r_send if right else l_send, recv_sem=z_recv.at[(dz + right) * chunks + q],
            device_id=(me + nx if right else me - nx, tp), device_id_type=MESH,
        )

    def z_total(n, right):
        return pltpu.make_async_remote_copy(
            src_ref=sent.at[pl.ds(0, n)], dst_ref=got.at[pl.ds(0, n)],
            send_sem=r_send if right else l_send, recv_sem=z_recv.at[0],
            device_id=(me, tp), device_id_type=MESH,
        )

    blocks_per = piece // side_rows

    def multiply(q):
        down = jnp.concatenate(
            [
                wall[:, down_at + p * pr : down_at + (p + 1) * pr, cols(q)].reshape(
                    piece_units, piece
                )
                for p in range(pieces)
            ]
            + [wall[:, down_at + routed :, cols(q)].reshape(shared_units, piece)],
            axis=0,
        )
        side_down = side[pl.ds(n_ep + q * blocks_per, blocks_per)].reshape(piece, side_cols)

        def product(j, half):
            at = tile_rows(half * nx + j)
            return jnp.dot(hidden[at], down, preferred_element_type=jnp.float32) + nt(
                side_hid[at], side_down
            )

        def leave(j, k):
            go = lambda: x_copy(q, j, k).start()
            over = lambda: h_copy(k, q).start()
            if hyb and k == 3 and q % 2:
                when([ends], over)
            elif hyb and k == 2:
                when([ends], go)
                when([inner], over)
            elif hyb and k == 0:
                when([inner], go)
            else:
                go()

        for half in reversed(range(nz // 2)):
            for j in range(1, nx):
                value = product(j, half).astype(jnp.bfloat16)
                for i in (1, 0):
                    k = 2 * half + i
                    xs[x_index(j, k, q)] = value[i * rows : (i + 1) * rows]
                    leave(j, k)
        for half in reversed(range(nz // 2)):
            value = product(0, half)
            for i in range(2):
                acc[(2 * half + i) * chunks + q] = value[i * rows : (i + 1) * rows]

    def relay(q):
        def pass_on(k):
            h_copy(k, q).wait_recv()
            i = x_index(1, k, q)
            value = xs[i].astype(jnp.float32) + hgot[q].astype(jnp.float32)
            xs[i] = value.astype(jnp.bfloat16)
            x_copy(q, 1, k).start()

        if hyb:
            when([ends], lambda: pass_on(0))
            if q % 2:
                when([inner], lambda: pass_on(3))

    def fold(q, k):
        conds = []
        if hyb and k == 3 and q % 2:
            conds = [inner]
        if hyb and k == 2:
            conds = [ends]

        def add():
            value = acc[k * chunks + q]
            for j in range(1, nx):
                x_copy(q, j, k).wait_recv()
                value = value + xr[x_index(j, k, q)].astype(jnp.float32)
            acc[k * chunks + q] = value

        when(conds, add)

    def reduce(q):
        for k in range(nz - 1, 0, -1):
            fold(q, k)
            dz = by_z([near[zz][k] for zz in range(nz)])

            def move(right, far, k=k, dz=dz):
                def act():
                    value = acc[k * chunks + q]
                    mine = dz * chunks + q

                    @pl.when(z == far)
                    def _():
                        sent[mine] = value.astype(jnp.bfloat16)

                    @pl.when(z != far)
                    def _():
                        z_copy(q, dz, right).wait_recv()
                        more = got[(dz + right) * chunks + q].astype(jnp.float32)
                        sent[mine] = (value + more).astype(jnp.bfloat16)

                    z_copy(q, dz, right).start()

                return act

            when([lambda: flag([near[zz][k] > zz for zz in range(nz)])], move(1, 0))
            when([lambda: flag([near[zz][k] < zz for zz in range(nz)])], move(0, nz - 1))
        fold(q, 0)

    def settle(q):
        @pl.when(z > 0)
        def _():
            z_copy(q, z, 1).wait_recv()
            acc[q] += got[(z + 1) * chunks + q].astype(jnp.float32)

        @pl.when(z < nz - 1)
        def _():
            z_copy(q, z, 0).wait_recv()
            acc[q] += got[z * chunks + q].astype(jnp.float32)

        out_ref[:, cols(q)] = acc[q].astype(jnp.bfloat16)

    for i in range(chunks + ahead):
        if i < chunks:
            arrive(pieces + i)
            multiply(i)
        if 0 < i <= chunks:
            relay(i - 1)
        if i >= ahead:
            reduce(i - ahead)
    for q in range(chunks):
        settle(q)

    for conds, copy in log:
        when(conds, lambda: copy().wait_send())
    each_own(lambda way: w_copy(None, y, way), finish)
    for step in range(1, ny):
        each_forward(lambda b, way: w_copy(None, b, way), step, finish, lambda b: None)
    side_all().wait_send()
    swap_copy(c).wait_send()
    aux_all().wait_send()
    count = (nx - 1) * nz * chunks
    if hyb:
        when([ends], lambda: x_total(count - chunks // 2).wait_send())
        when([inner], lambda: x_total(count - chunks).wait_send())
        when([ends], lambda: h_total(chunks // 2).wait_send())
        when([inner], lambda: h_total(chunks).wait_send())
    else:
        x_total(count).wait_send()
    for zz in range(nz):
        if zz < nz - 1:
            pl.when(z == zz)(lambda: z_total((nz - 1 - zz) * chunks, 1).wait_send())
        if zz > 0:
            pl.when(z == zz)(lambda: z_total(zz * chunks, 0).wait_send())


def body(
    nx,
    nc,
    tokens,
    norm_gain,
    expert_ids,
    route_weights,
    expert_gate,
    expert_up,
    expert_down,
    shared_gate,
    shared_up,
    shared_down,
    side_in,
    side_out,
    side_gate,
):
    tok_count, width = tokens.shape
    n_ep, n_tp = lax.axis_size("ep"), lax.axis_size("tp")
    nz, ny = n_ep // nx, n_tp // nc
    me = lax.axis_index("ep")
    local_experts, ff_part, _ = expert_gate.shape
    routed = local_experts * ff_part
    shared_rows = shared_gate.shape[0] // n_ep
    side_rows, side_all = side_in.shape
    side_cols = side_all // n_ep
    chunks = 8
    ahead = 3
    pieces = 2 * local_experts
    piece = width // chunks
    extra = -(-shared_rows // 16) * 16
    padded = -(-tok_count // 128) * 128

    def shared_part(array):
        if shared_rows % 16 == 0:
            return array
        own = lax.dynamic_slice_in_dim(array, me * shared_rows, shared_rows, 0)
        return jnp.pad(own, ((0, extra - shared_rows), (0, 0)))

    def side_part(array):
        if side_cols % 128 == 0:
            return array
        return array.reshape(side_rows, n_ep, side_cols).transpose(1, 0, 2)

    bf16, f32 = jnp.bfloat16, jnp.float32
    dma = pltpu.SemaphoreType.DMA
    dims = (nz, nx, ny, nc, local_experts, pieces, extra, chunks, ahead)
    return pl.pallas_call(
        functools.partial(kernel, dims),
        out_shape=jax.ShapeDtypeStruct((tok_count, width), bf16),
        in_specs=[pl.BlockSpec(memory_space=pltpu.VMEM)] * 5
        + [pl.BlockSpec(memory_space=pl.ANY)] * 8,
        out_specs=pl.BlockSpec(memory_space=pltpu.VMEM),
        scratch_shapes=[
            pltpu.VMEM((n_ep * tok_count, width), bf16),
            pltpu.VMEM((n_tp, 3 * (routed + extra), width), bf16),
            pltpu.VMEM((2 * n_ep, side_rows, side_cols), bf16),
            pltpu.VMEM((n_ep * tok_count, n_tp * (routed + extra)), bf16),
            pltpu.VMEM((n_ep * tok_count, side_cols), bf16),
            pltpu.VMEM((nz * chunks, tok_count, piece), f32),
            pltpu.VMEM(((nx - 1) * nz * chunks, tok_count, piece), bf16),
            pltpu.VMEM(((nx - 1) * nz * chunks, tok_count, piece), bf16),
            pltpu.VMEM((nz * chunks, tok_count, piece), bf16),
            pltpu.VMEM(((nz + 1) * chunks, tok_count, piece), bf16),
            pltpu.VMEM((chunks if nx == 2 else 1, tok_count, piece), bf16),
            pltpu.VMEM((n_ep, 8, padded), f32),
            pltpu.VMEM((n_ep, 8, padded), f32),
            pltpu.VMEM((n_ep * tok_count, 8), f32),
            dma((nz, 1 + nx, 2)),
            dma((n_ep, 2)),
            dma((2,)),
            dma((ny, 1 + nc)),
            dma((pieces + chunks, n_tp)),
            dma,
            dma,
            dma,
            dma,
            dma((2,)),
            dma,
            dma,
            dma,
            dma(((nx - 1) * nz * chunks,)),
            dma,
            dma,
            dma(((nz + 1) * chunks,)),
            dma,
            dma((chunks,)),
        ],
        compiler_params=pltpu.CompilerParams(
            collective_id=0, has_side_effects=True, vmem_limit_bytes=63000 * 1024
        ),
        name="layer",
    )(
        tokens, norm_gain[None, :], expert_ids.T, route_weights.T, side_gate.reshape(-1, 128),
        expert_gate.reshape(routed, width), expert_up.reshape(routed, width),
        expert_down.reshape(routed, width), shared_part(shared_gate), shared_part(shared_up),
        shared_part(shared_down), side_part(side_in), side_part(side_out),
    )


def solution(mesh):
    devices = mesh.devices
    nx = len({d.coords[0] for d in devices[:, 0]})
    nc = len({d.core_on_chip for d in devices[0, :]})
    placed = (
        P(("ep", "tp"), None),
        P(),
        P(("ep", "tp"), None),
        P(("ep", "tp"), None),
        P("ep", "tp", None),
        P("ep", "tp", None),
        P("ep", "tp", None),
        P("tp", None),
        P("tp", None),
        P("tp", None),
        P("ep", None),
        P("ep", None),
        P(),
    )
    return jax.shard_map(
        functools.partial(body, nx, nc),
        mesh=mesh,
        in_specs=placed,
        out_specs=P(("ep", "tp"), None),
        check_vma=False,
    )
```

```python
import functools

import jax
import jax.numpy as jnp
from jax import lax
from jax.experimental import pallas as pl
from jax.experimental.pallas import tpu as pltpu
from jax.sharding import PartitionSpec as P

norm_eps = 1.0
MESH = pl.DeviceIdType.MESH
NT = (((1,), (1,)), ((), ()))


def silu(v):
    return v / (1.0 + jnp.exp(-v))


def when(conds, act):
    conds = [cond() for cond in conds]
    if any(cond is False for cond in conds):
        return
    conds = [cond for cond in conds if cond is not True]
    if not conds:
        act()
        return
    both = conds[0]
    for cond in conds[1:]:
        both = jnp.logical_and(both, cond)
    pl.when(both)(act)


def kernel(
    dims,
    tokens_ref, gain_ref, ids_ref, route_ref, side_gate_ref,
    gate_ref, up_ref, down_ref, s_gate_ref, s_up_ref, s_down_ref, side_in_ref, side_out_ref,
    out_ref,
    tok, wall, side, hidden, side_hid, acc, xs, xr, sent, got, hgot, saux, sc, scol,
    tok_send, tok_recv, hyb_send, w_send, w_recv, side_send, side_recv, swap_send, swap_recv,
    local_sem, aux_send, aux_recv, x_send, x_recv, r_send, l_send, z_recv, h_send, h_recv,
):
    nz, nx, ny, nc, local_experts, pieces, extra, chunks = dims
    n_ep, n_tp = nz * nx, ny * nc
    me, tp = lax.axis_index("ep"), lax.axis_index("tp")
    z, x = me // nx, me % nx
    y, c = tp // nc, tp % nc
    rows, width = tokens_ref.shape
    routed = gate_ref.shape[0]
    pr = routed // pieces
    per_expert = pieces // local_experts
    piece_units, shared_units = n_tp * pr, n_tp * extra
    side_rows, side_cols = side.shape[1:]
    piece = width // chunks
    unit_w = width // 16
    edges = [0, 5 * unit_w, 10 * unit_w, width]
    parts = len(edges) - 1
    down_at = 2 * (routed + extra)
    tile = 2 * rows
    hyb = nx == 2 and nz == 4
    tiles = n_ep // 2

    near = [
        sorted(range(nz), key=lambda b: (abs(b - zz), -b if 2 * zz < nz else b))
        for zz in range(nz)
    ]
    place_of = [[near[zz].index(b) for b in range(nz)] for zz in range(nz)]

    def by_z(values):
        out = values[0]
        if all(v == out for v in values):
            return out
        for zz in range(1, nz):
            out = jnp.where(z == zz, values[zz], out)
        return out

    def flag(values):
        values = [bool(v) for v in values]
        if all(values) or not any(values):
            return values[0]
        return by_z([int(v) for v in values]) == 1

    ends = lambda: flag([zz in (0, nz - 1) for zz in range(nz)])
    inner = lambda: flag([zz not in (0, nz - 1) for zz in range(nz)])
    twin = z + 1 - 2 * (z % 2)

    def slot(j, k):
        return k // 2 * (2 * nx) + 2 * j + k % 2

    def cols(q):
        return pl.ds(q * piece, piece)

    barrier = pltpu.get_barrier_semaphore()
    for j in range(1, n_ep):
        pl.semaphore_signal(barrier, inc=1, device_id=((me + j) % n_ep, tp), device_id_type=MESH)
    for j in range(1, n_tp):
        pl.semaphore_signal(barrier, inc=1, device_id=(me, (tp + j) % n_tp), device_id_type=MESH)


    def slot_rows(s):
        return pl.ds(s * rows if isinstance(s, int) else pl.multiple_of(s * rows, 16), rows)

    def tok_copy(from_slot, to_slot, h, target, send):
        part = pl.ds(edges[h], edges[h + 1] - edges[h])
        return pltpu.make_async_remote_copy(
            src_ref=tok.at[slot_rows(from_slot), part],
            dst_ref=tok.at[slot_rows(to_slot), part],
            send_sem=send, recv_sem=tok_recv.at[to_slot, h],
            device_id=target, device_id_type=MESH,
        )

    def tok_wait(s, h):
        tok_copy(s, s, h, (me, tp), tok_send.at[0, 0, 0]).wait_recv()

    def along(k, h, d):
        to = by_z([
            place_of[zz + d][near[zz][k]] if 0 <= zz + d < nz else 0 for zz in range(nz)
        ])
        return tok_copy(
            slot(0, k), slot(0, to), h, (me + d * nx, tp), tok_send.at[k, (1 - d) // 2, h]
        )

    def across(k, h, j):
        return tok_copy(
            slot(0, k), slot(nx - j, k), h, (z * nx + (x + j) % nx, tp), tok_send.at[k, 1 + j, h]
        )

    def onward(k, to, h):
        return tok_copy(
            slot(1, k), slot(1, to), h, (me + (twin - z) * nx, tp), hyb_send.at[h]
        )

    def crosses(k, h):
        if hyb and k == nz - 1 and h == parts - 1:
            return inner
        if hyb and k == nz - 2:
            return ends
        return lambda: True

    log = []

    def launch(conds, copy):
        log.append((conds, copy))
        when(conds, lambda: copy().start())

    def send_block(conds, k, h):
        bind = functools.partial
        for d in (1, -1):
            goes = [
                0 <= zz + d < nz and (near[zz][k] - zz) * d <= 0 for zz in range(nz)
            ]
            launch(conds + [lambda goes=goes: flag(goes)], bind(along, k, h, d))
        for j in range(1, nx):
            launch(conds + [crosses(k, h)], bind(across, k, h, j))

    def stage(step, h):
        for k in range(1, nz):
            here = [abs(near[zz][k] - zz) == step for zz in range(nz)]
            if any(here):
                cond = lambda here=here: flag(here)
                when([cond], lambda: tok_wait(slot(0, k), h))
                send_block([cond], k, h)
        if hyb and step == 1:
            tok_wait(slot(1, 0), h)
            launch([ends], functools.partial(onward, 0, nz - 2, h))
        if hyb and step == nz - 1 and h == parts - 1:
            when([inner], lambda: tok_wait(slot(1, nz - 1), h))
            launch([inner], functools.partial(onward, nz - 1, nz - 1, h))

    def cross_wait(half):
        for j in range(1, nx):
            for k in (2 * half, 2 * half + 1):
                for h in range(parts):
                    if hyb and k == 0:
                        continue
                    conds = [ends] if hyb and k == nz - 1 and h == parts - 1 else []
                    when(conds, lambda: tok_wait(slot(j, k), h))


    shared_at = pl.ds(0, extra)
    if s_gate_ref.shape[0] > extra:
        shared_at = pl.ds(pl.multiple_of(me * extra, extra), extra)

    def w_parts(k):
        slab = wall.at[tp]
        if k < pieces:
            at, r0 = pl.ds(k * pr, pr), 2 * extra + 2 * k * pr
            parts = [
                (gate_ref.at[at], slab.at[pl.ds(r0, pr)]),
                (up_ref.at[at], slab.at[pl.ds(r0 + pr, pr)]),
            ]
            if k == 0:
                parts += [
                    (s_gate_ref.at[shared_at], slab.at[pl.ds(0, extra)]),
                    (s_up_ref.at[shared_at], slab.at[pl.ds(extra, extra)]),
                ]
            return parts
        q = cols(k - pieces)
        return [
            (down_ref.at[:, q], slab.at[pl.ds(down_at, routed), q]),
            (s_down_ref.at[shared_at, q], slab.at[pl.ds(down_at + routed, extra), q]),
        ]

    def w_place(k, owner):
        if k == 0:
            return wall.at[owner, pl.ds(0, 2 * (extra + pr))]
        if k < pieces:
            return wall.at[owner, pl.ds(2 * (extra + k * pr), 2 * pr)]
        return wall.at[owner, pl.ds(down_at, routed + extra), cols(k - pieces)]

    def w_copy(k, by, way, refs=None):
        if way < 2:
            target = (me, tp + nc if way == 0 else tp - nc)
        else:
            target = (me, y * nc + (c + way - 1) % nc)
        owner = by * nc + c
        if refs is None:
            refs = (wall.at[owner],) * 2 if k is None else (w_place(k, owner),) * 2
        return pltpu.make_async_remote_copy(
            src_ref=refs[0], dst_ref=refs[1], send_sem=w_send.at[by, way],
            recv_sem=w_recv.at[0 if k is None else k, owner],
            device_id=target, device_id_type=MESH,
        )

    def w_wait(k, owner):
        pltpu.make_async_remote_copy(
            src_ref=w_place(k, owner), dst_ref=w_place(k, owner), send_sem=w_send.at[0, 0],
            recv_sem=w_recv.at[k, owner], device_id=(me, tp), device_id_type=MESH,
        ).wait_recv()

    def each_own(copy_of, act):
        pl.when(y < ny - 1)(lambda: act(copy_of(0)))
        pl.when(y > 0)(lambda: act(copy_of(1)))
        for way in range(2, 1 + nc):
            act(copy_of(way))

    def each_forward(copy_of, step, act, arrive):
        @pl.when(y >= step)
        def _():
            b = y - step
            arrive(b)
            pl.when(y < ny - 1)(lambda: act(copy_of(b, 0)))
            for way in range(2, 1 + nc):
                act(copy_of(b, way))

        @pl.when(y + step <= ny - 1)
        def _():
            b = y + step
            arrive(b)
            pl.when(y > 0)(lambda: act(copy_of(b, 1)))
            for way in range(2, 1 + nc):
                act(copy_of(b, way))

    start = lambda copy: copy.start()
    finish = lambda copy: copy.wait_send()

    def w_gathered(k):
        for step in range(1, ny):
            each_forward(
                lambda b, way: w_copy(k, b, way), step, start, lambda b: w_wait(k, b * nc + c)
            )

    def w_across(k):
        for j in range(1, nc):
            for by in range(ny):
                w_wait(k, by * nc + (c + j) % nc)


    def side_source(ref, to):
        if len(ref.shape) == 3:
            return ref.at[to]
        return ref.at[:, pl.ds(pl.multiple_of(to * side_cols, side_cols), side_cols)]

    def side_copy(j, p):
        to = (me + j) % n_ep
        return pltpu.make_async_remote_copy(
            src_ref=side_source((side_in_ref, side_out_ref)[p], to),
            dst_ref=side.at[p * n_ep + me],
            send_sem=side_send, recv_sem=side_recv, device_id=(to, tp), device_id_type=MESH,
        )

    def side_all():
        whole = side.at[pl.ds(0, n_ep - 1)]
        return pltpu.make_async_remote_copy(
            src_ref=whole, dst_ref=whole, send_sem=side_send, recv_sem=side_recv,
            device_id=(me, tp), device_id_type=MESH,
        )

    def side_own(p):
        return pltpu.make_async_copy(
            side_source((side_in_ref, side_out_ref)[p], me), side.at[p * n_ep + me],
            local_sem.at[1],
        )

    def swap_copy(half):
        part = side.at[pl.ds(half * n_ep, n_ep)]
        return pltpu.make_async_remote_copy(
            src_ref=part, dst_ref=part, send_sem=swap_send, recv_sem=swap_recv,
            device_id=(me, y * nc + 1 - c), device_id_type=MESH,
        )


    def aux_copy(k, j):
        to = by_z([near[zz][k] for zz in range(nz)]) * nx + (x + j) % nx
        k_there = by_z([place_of[near[zz][k]][zz] for zz in range(nz)])
        return pltpu.make_async_remote_copy(
            src_ref=saux.at[to], dst_ref=sc.at[slot((nx - j) % nx, k_there)],
            send_sem=aux_send, recv_sem=aux_recv, device_id=(to, tp), device_id_type=MESH,
        )

    def aux_all():
        return pltpu.make_async_remote_copy(
            src_ref=saux.at[pl.ds(0, n_ep - 1)], dst_ref=sc.at[pl.ds(0, n_ep - 1)],
            send_sem=aux_send, recv_sem=aux_recv, device_id=(me, tp), device_id_type=MESH,
        )

    for k in range(pieces + chunks):
        for part in w_parts(k):
            pltpu.make_async_copy(*part, local_sem.at[0]).start()
    for p in range(nc):
        pl.when(c == p)(lambda: side_own(p).start())

    values = tokens_ref[...].astype(jnp.float32)
    scale_inv = lax.rsqrt(jnp.mean(values * values, axis=-1, keepdims=True) + norm_eps)
    normed = (values * scale_inv * gain_ref[...]).astype(jnp.bfloat16)
    tok[slot_rows(0), :] = normed

    pl.semaphore_wait(barrier, n_ep + n_tp - 2)
    for p in range(nc):
        def side_go(p=p):
            for j in range(1, n_ep):
                side_copy(j, p).start()

        pl.when(c == p)(side_go)
    for h in range(parts):
        send_block([], 0, h)
    for k in range(pieces + chunks):
        for refs in w_parts(k):
            each_own(lambda way: w_copy(k, y, way, refs), start)

    side_vector = side_gate_ref[...].astype(jnp.float32)
    lanes = side_vector.shape[1]
    side_vector = jnp.concatenate(
        [jnp.broadcast_to(side_vector[i : i + 1], (8, lanes)) for i in range(width // lanes)],
        axis=1,
    ).astype(jnp.bfloat16)
    opening = lax.dot_general(side_vector, normed, NT, preferred_element_type=jnp.float32)
    opening = 1.0 / (1.0 + jnp.exp(-opening))
    ids, route = ids_ref[...], route_ref[...]
    row = lax.broadcasted_iota(jnp.int32, (8, rows), 0)
    for to in range(n_ep):
        block = jnp.where(row == local_experts, opening, 0.0)
        for e in range(local_experts):
            hit = jnp.where(ids == to * local_experts + e, route, 0.0)
            block = jnp.where(row == e, jnp.sum(hit, axis=0, keepdims=True), block)
        gap = sc.shape[2] - rows
        saux[to] = jnp.concatenate([block, jnp.zeros((8, gap), jnp.float32)], axis=1)
    sc[0] = saux[me]
    for k in range(nz):
        for j in range(nx):
            if k or j:
                aux_copy(k, j).start()


    def tile_rows(t):
        return pl.ds(pl.multiple_of(t * tile, 16), tile)

    def column(at, n):
        picked = scol[at, :]
        lane = lax.broadcasted_iota(jnp.int32, picked.shape, 1)
        return jnp.sum(jnp.where(lane == n, picked, 0.0), axis=1, keepdims=True)

    def nt(a, b):
        return lax.dot_general(a, b, NT, preferred_element_type=jnp.float32)

    def unit(t, p):
        at = tile_rows(t)
        r0 = 2 * extra + p * (2 * pr)
        if not isinstance(p, int):
            r0 = pl.multiple_of(r0, 16)
        a = tok[at, :]
        gate = wall[:, pl.ds(r0, pr), :].reshape(piece_units, width)
        up = wall[:, pl.ds(r0 + pr, pr), :].reshape(piece_units, width)
        gated = silu(nt(a, gate)) * nt(a, up) * column(at, p // per_expert)
        to = p * piece_units if isinstance(p, int) else pl.multiple_of(p * piece_units, 128)
        hidden[at, pl.ds(to, piece_units)] = gated.astype(jnp.bfloat16)

    def units(t0, t1, p0, p1):
        n = p1 - p0
        if (t1 - t0) * n > 0:
            def step(i, carry):
                unit(t0 + i // n, p0 + i % n)
                return carry

            lax.fori_loop(0, (t1 - t0) * n, step, 0)

    def extras(t0, t1):
        def step(t, carry):
            at = tile_rows(t)
            a = tok[at, :]
            both = jnp.concatenate([
                wall[:, :extra, :].reshape(shared_units, width),
                wall[:, extra : 2 * extra, :].reshape(shared_units, width),
            ], axis=0)
            both = nt(a, both)
            gated = silu(both[:, :shared_units]) * both[:, shared_units:]
            hidden[at, pieces * piece_units :] = gated.astype(jnp.bfloat16)
            side_part = jnp.dot(
                a, side[:n_ep].reshape(width, side_cols), preferred_element_type=jnp.float32
            )
            side_hid[at] = (silu(side_part) * column(at, local_experts)).astype(jnp.bfloat16)
            return carry

        lax.fori_loop(t0, t1, step, 0)

    for h in range(parts):
        stage(1, h)
    pltpu.make_async_copy(wall.at[tp], wall.at[tp], local_sem.at[0]).wait()
    w_gathered(0)
    aux_all().wait_recv()
    for s in range(n_ep):
        scol[slot_rows(s), :] = sc[s].T[:rows]
    w_across(0)
    units(0, 1, 0, 1)
    for h in range(parts - 1):
        stage(2, h)
    w_gathered(1)
    stage(2, parts - 1)
    w_across(1)
    units(0, 1, 1, 2)
    cross_wait(0)
    units(1, nx, 0, 2)
    for s in range(3, nz):
        for h in range(parts - 1):
            stage(s, h)
    for p in range(2, pieces - 1):
        w_gathered(p)
    for p in range(nc):
        pl.when(c == p)(lambda: side_own(p).wait())
    side_all().wait_recv()
    swap_copy(c).start()
    for p in range(2, pieces - 1):
        w_across(p)
    units(0, nx, 2, pieces - 1)
    for s in range(3, nz):
        stage(s, parts - 1)
    units(nx, nx + 1, 0, pieces - 1)
    w_gathered(pieces - 1)
    swap_copy(1 - c).wait_recv()
    extras(0, nx + 1)
    w_across(pieces - 1)
    units(0, nx + 1, pieces - 1, pieces)
    w_gathered(pieces)
    for half in range(1, nz // 2):
        cross_wait(half)
    units(nx + 1, tiles, 0, pieces)
    w_gathered(pieces + 1)
    w_across(pieces)


    def x_index(j, k, q):
        return ((j - 1) * nz + k) * chunks + q

    def x_copy(q, j, k):
        i = x_index(j, k, q)
        return pltpu.make_async_remote_copy(
            src_ref=xs.at[i], dst_ref=xr.at[i], send_sem=x_send, recv_sem=x_recv.at[i],
            device_id=(z * nx + (x + j) % nx, tp), device_id_type=MESH,
        )

    def x_total(n):
        return pltpu.make_async_remote_copy(
            src_ref=xs.at[pl.ds(0, n)], dst_ref=xr.at[pl.ds(0, n)], send_sem=x_send,
            recv_sem=x_recv.at[0], device_id=(me, tp), device_id_type=MESH,
        )

    def h_copy(k, q):
        return pltpu.make_async_remote_copy(
            src_ref=xs.at[x_index(1, k, q)], dst_ref=hgot.at[q], send_sem=h_send,
            recv_sem=h_recv.at[q], device_id=(me + (twin - z) * nx, tp), device_id_type=MESH,
        )

    def h_total(n):
        return pltpu.make_async_remote_copy(
            src_ref=xs.at[pl.ds(0, n)], dst_ref=hgot.at[pl.ds(0, n)], send_sem=h_send,
            recv_sem=h_recv.at[0], device_id=(me, tp), device_id_type=MESH,
        )

    def z_copy(q, dz, right):
        return pltpu.make_async_remote_copy(
            src_ref=sent.at[dz * chunks + q], dst_ref=got.at[(dz + right) * chunks + q],
            send_sem=r_send if right else l_send, recv_sem=z_recv.at[(dz + right) * chunks + q],
            device_id=(me + nx if right else me - nx, tp), device_id_type=MESH,
        )

    def z_total(n, right):
        return pltpu.make_async_remote_copy(
            src_ref=sent.at[pl.ds(0, n)], dst_ref=got.at[pl.ds(0, n)],
            send_sem=r_send if right else l_send, recv_sem=z_recv.at[0],
            device_id=(me, tp), device_id_type=MESH,
        )

    blocks_per = piece // side_rows

    def product(q, j, half):
        down = jnp.concatenate(
            [
                wall[:, down_at + p * pr : down_at + (p + 1) * pr, cols(q)].reshape(
                    piece_units, piece
                )
                for p in range(pieces)
            ]
            + [wall[:, down_at + routed :, cols(q)].reshape(shared_units, piece)],
            axis=0,
        )
        side_down = side[pl.ds(n_ep + q * blocks_per, blocks_per)].reshape(piece, side_cols)
        at = tile_rows(half * nx + j)
        return jnp.dot(hidden[at], down, preferred_element_type=jnp.float32) + nt(
            side_hid[at], side_down
        )

    def detour(q, k):
        return hyb and k == 3 and q < chunks // 2

    def leave(q, j, k):
        go = lambda: x_copy(q, j, k).start()
        if detour(q, k):
            when([ends], lambda: h_copy(k, q).start())
        elif hyb and k == 2:
            when([ends], go)
        elif hyb and k == 0:
            when([inner], go)
        else:
            go()

    def partial_sum(q, half, j):
        value = product(q, j, half).astype(jnp.bfloat16)
        for i in (1, 0):
            k = 2 * half + i
            xs[x_index(j, k, q)] = value[i * rows : (i + 1) * rows]
            if q < chunks // 2 or k == nz - 1:
                leave(q, j, k)
            if hyb and k == 2:
                when([inner], lambda: h_copy(k, q).start())

    def own_sum(q, half):
        value = product(q, 0, half)
        for i in range(2):
            acc[(2 * half + i) * chunks + q] = value[i * rows : (i + 1) * rows]

    def relay(q):
        def pass_on(k):
            h_copy(k, q).wait_recv()
            i = x_index(1, k, q)
            value = xs[i].astype(jnp.float32) + hgot[q].astype(jnp.float32)
            xs[i] = value.astype(jnp.bfloat16)
            x_copy(q, 1, k).start()

        if hyb:
            when([ends], lambda: pass_on(0))
            if detour(q, 3):
                when([inner], lambda: pass_on(3))

    def fold(q, k):
        conds = []
        if detour(q, k):
            conds = [inner]
        if hyb and k == 2:
            conds = [ends]

        def add():
            value = acc[k * chunks + q]
            for j in range(1, nx):
                x_copy(q, j, k).wait_recv()
                value = value + xr[x_index(j, k, q)].astype(jnp.float32)
            acc[k * chunks + q] = value

        when(conds, add)

    def move_on(q, k):
        fold(q, k)
        dz = by_z([near[zz][k] for zz in range(nz)])

        def move(right, far):
            def act():
                value = acc[k * chunks + q]
                mine = dz * chunks + q

                @pl.when(z == far)
                def _():
                    sent[mine] = value.astype(jnp.bfloat16)

                @pl.when(z != far)
                def _():
                    z_copy(q, dz, right).wait_recv()
                    more = got[(dz + right) * chunks + q].astype(jnp.float32)
                    sent[mine] = (value + more).astype(jnp.bfloat16)

                z_copy(q, dz, right).start()

            return act

        when([lambda: flag([near[zz][k] > zz for zz in range(nz)])], move(1, 0))
        when([lambda: flag([near[zz][k] < zz for zz in range(nz)])], move(0, nz - 1))

    def settle(q):
        fold(q, 0)

        @pl.when(z > 0)
        def _():
            z_copy(q, z, 1).wait_recv()
            acc[q] += got[(z + 1) * chunks + q].astype(jnp.float32)

        @pl.when(z < nz - 1)
        def _():
            z_copy(q, z, 0).wait_recv()
            acc[q] += got[z * chunks + q].astype(jnp.float32)

        out_ref[:, cols(q)] = acc[q].astype(jnp.bfloat16)

    for j in range(1, nx):
        partial_sum(0, 0, j)
    extras(nx + 1, tiles)

    halves = nz // 2
    first = chunks // 2
    late = range(first, chunks)

    def sums(q):
        if q:
            w_across(pieces + q)
        for half in reversed(range(halves)):
            for j in range(1, nx):
                if q or half:
                    partial_sum(q, half, j)
        for half in reversed(range(halves)):
            own_sum(q, half)

    def move_all(q):
        for k in range(nz - 1, 0, -1):
            move_on(q, k)

    gather = lambda q: w_gathered(pieces + q)
    gather(2)
    sums(0)
    sums(1)
    relay(0)
    gather(3)
    sums(2)
    relay(1)
    sums(3)
    relay(2)
    gather(4)
    move_all(0)
    sums(4)
    gather(5)
    relay(3)
    move_all(1)
    gather(6)
    sums(5)
    sums(6)
    gather(7)
    move_all(2)
    sums(7)
    for k in range(nz - 2, -1, -1):
        for q in late:
            for j in range(1, nx):
                leave(q, j, k)
            if k == 0:
                relay(q)
    for q in range(3, first):
        move_all(q)
    for k in range(nz - 1, 0, -1):
        for q in late:
            move_on(q, k)
        if k == nz - 1:
            settle(0)
            settle(1)
        elif k == nz - 2:
            for q in range(2, first):
                settle(q)
    for q in late:
        settle(q)

    for conds, copy in log:
        when(conds, lambda: copy().wait_send())
    each_own(lambda way: w_copy(None, y, way), finish)
    for step in range(1, ny):
        each_forward(lambda b, way: w_copy(None, b, way), step, finish, lambda b: None)
    side_all().wait_send()
    swap_copy(c).wait_send()
    aux_all().wait_send()
    count = (nx - 1) * nz * chunks
    if hyb:
        when([ends], lambda: x_total(count - chunks // 2).wait_send())
        when([inner], lambda: x_total(count - chunks).wait_send())
        when([ends], lambda: h_total(chunks // 2).wait_send())
        when([inner], lambda: h_total(chunks).wait_send())
    else:
        x_total(count).wait_send()
    for zz in range(nz):
        if zz < nz - 1:
            pl.when(z == zz)(lambda: z_total((nz - 1 - zz) * chunks, 1).wait_send())
        if zz > 0:
            pl.when(z == zz)(lambda: z_total(zz * chunks, 0).wait_send())


def body(
    nx,
    nc,
    tokens,
    norm_gain,
    expert_ids,
    route_weights,
    expert_gate,
    expert_up,
    expert_down,
    shared_gate,
    shared_up,
    shared_down,
    side_in,
    side_out,
    side_gate,
):
    tok_count, width = tokens.shape
    n_ep, n_tp = lax.axis_size("ep"), lax.axis_size("tp")
    nz, ny = n_ep // nx, n_tp // nc
    me = lax.axis_index("ep")
    local_experts, ff_part, _ = expert_gate.shape
    routed = local_experts * ff_part
    shared_rows = shared_gate.shape[0] // n_ep
    side_rows, side_all = side_in.shape
    side_cols = side_all // n_ep
    chunks = 8
    pieces = 2 * local_experts
    piece = width // chunks
    extra = -(-shared_rows // 16) * 16
    padded = -(-tok_count // 128) * 128

    def shared_part(array):
        if shared_rows % 16 == 0:
            return array
        own = lax.dynamic_slice_in_dim(array, me * shared_rows, shared_rows, 0)
        return jnp.pad(own, ((0, extra - shared_rows), (0, 0)))

    def side_part(array):
        if side_cols % 128 == 0:
            return array
        return array.reshape(side_rows, n_ep, side_cols).transpose(1, 0, 2)

    bf16, f32 = jnp.bfloat16, jnp.float32
    dma = pltpu.SemaphoreType.DMA
    dims = (nz, nx, ny, nc, local_experts, pieces, extra, chunks)
    return pl.pallas_call(
        functools.partial(kernel, dims),
        out_shape=jax.ShapeDtypeStruct((tok_count, width), bf16),
        in_specs=[pl.BlockSpec(memory_space=pltpu.VMEM)] * 5
        + [pl.BlockSpec(memory_space=pl.ANY)] * 8,
        out_specs=pl.BlockSpec(memory_space=pltpu.VMEM),
        scratch_shapes=[
            pltpu.VMEM((n_ep * tok_count, width), bf16),
            pltpu.VMEM((n_tp, 3 * (routed + extra), width), bf16),
            pltpu.VMEM((2 * n_ep, side_rows, side_cols), bf16),
            pltpu.VMEM((n_ep * tok_count, n_tp * (routed + extra)), bf16),
            pltpu.VMEM((n_ep * tok_count, side_cols), bf16),
            pltpu.VMEM((nz * chunks, tok_count, piece), f32),
            pltpu.VMEM(((nx - 1) * nz * chunks, tok_count, piece), bf16),
            pltpu.VMEM(((nx - 1) * nz * chunks, tok_count, piece), bf16),
            pltpu.VMEM((nz * chunks, tok_count, piece), bf16),
            pltpu.VMEM(((nz + 1) * chunks, tok_count, piece), bf16),
            pltpu.VMEM((chunks if nx == 2 else 1, tok_count, piece), bf16),
            pltpu.VMEM((n_ep, 8, padded), f32),
            pltpu.VMEM((n_ep, 8, padded), f32),
            pltpu.VMEM((n_ep * tok_count, 8), f32),
            dma((nz, 1 + nx, 3)),
            dma((n_ep, 3)),
            dma((3,)),
            dma((ny, 1 + nc)),
            dma((pieces + chunks, n_tp)),
            dma,
            dma,
            dma,
            dma,
            dma((2,)),
            dma,
            dma,
            dma,
            dma(((nx - 1) * nz * chunks,)),
            dma,
            dma,
            dma(((nz + 1) * chunks,)),
            dma,
            dma((chunks,)),
        ],
        compiler_params=pltpu.CompilerParams(
            collective_id=0, has_side_effects=True, vmem_limit_bytes=63000 * 1024
        ),
        name="layer",
    )(
        tokens, norm_gain[None, :], expert_ids.T, route_weights.T, side_gate.reshape(-1, 128),
        expert_gate.reshape(routed, width), expert_up.reshape(routed, width),
        expert_down.reshape(routed, width), shared_part(shared_gate), shared_part(shared_up),
        shared_part(shared_down), side_part(side_in), side_part(side_out),
    )


def solution(mesh):
    devices = mesh.devices
    nx = len({d.coords[0] for d in devices[:, 0]})
    nc = len({d.core_on_chip for d in devices[0, :]})
    placed = (
        P(("ep", "tp"), None),
        P(),
        P(("ep", "tp"), None),
        P(("ep", "tp"), None),
        P("ep", "tp", None),
        P("ep", "tp", None),
        P("ep", "tp", None),
        P("tp", None),
        P("tp", None),
        P("tp", None),
        P("ep", None),
        P("ep", None),
        P(),
    )
    return jax.shard_map(
        functools.partial(body, nx, nc),
        mesh=mesh,
        in_specs=placed,
        out_specs=P(("ep", "tp"), None),
        check_vma=False,
    )
```

```python
import functools

import jax
import jax.numpy as jnp
from jax import lax
from jax.experimental import pallas as pl
from jax.experimental.pallas import tpu as pltpu
from jax.sharding import PartitionSpec as P

norm_eps = 1.0
MESH = pl.DeviceIdType.MESH
NT = (((1,), (1,)), ((), ()))


def silu(v):
    return v / (1.0 + jnp.exp(-v))


def when(conds, act):
    conds = [cond() for cond in conds]
    if any(cond is False for cond in conds):
        return
    conds = [cond for cond in conds if cond is not True]
    if not conds:
        act()
        return
    both = conds[0]
    for cond in conds[1:]:
        both = jnp.logical_and(both, cond)
    pl.when(both)(act)


def kernel(
    dims,
    tokens_ref, gain_ref, ids_ref, route_ref, side_gate_ref,
    gate_ref, up_ref, down_ref, s_gate_ref, s_up_ref, s_down_ref, side_in_ref, side_out_ref,
    out_ref,
    tok, wall, side, hidden, side_hid, acc, xs, xr, sent, got, hgot, saux, sc, scol, out_v,
    tok_send, tok_recv, hyb_send, w_send, w_recv, side_send, side_recv, swap_send, swap_recv,
    local_sem, aux_send, aux_recv, x_send, x_recv, r_send, l_send, z_recv, h_send, h_recv,
):
    nz, nx, ny, nc, local_experts, pieces, extra, chunks = dims
    n_ep, n_tp = nz * nx, ny * nc
    me, tp = lax.axis_index("ep"), lax.axis_index("tp")
    z, x = me // nx, me % nx
    y, c = tp // nc, tp % nc
    rows, width = tokens_ref.shape
    routed = gate_ref.shape[0]
    pr = routed // pieces
    per_expert = pieces // local_experts
    piece_units, shared_units = n_tp * pr, n_tp * extra
    side_rows, side_cols = side.shape[1:]
    piece = width // chunks
    unit_w = width // 16
    edges = [0, 5 * unit_w, 10 * unit_w, width]
    parts = len(edges) - 1
    down_at = 2 * (routed + extra)
    tile = 2 * rows
    hyb = nx == 2 and nz == 4
    tiles = n_ep // 2

    near = [
        sorted(range(nz), key=lambda b: (abs(b - zz), -b if 2 * zz < nz else b))
        for zz in range(nz)
    ]
    place_of = [[near[zz].index(b) for b in range(nz)] for zz in range(nz)]

    def by_z(values):
        out = values[0]
        if all(v == out for v in values):
            return out
        for zz in range(1, nz):
            out = jnp.where(z == zz, values[zz], out)
        return out

    def flag(values):
        values = [bool(v) for v in values]
        if all(values) or not any(values):
            return values[0]
        return by_z([int(v) for v in values]) == 1

    ends = lambda: flag([zz in (0, nz - 1) for zz in range(nz)])
    inner = lambda: flag([zz not in (0, nz - 1) for zz in range(nz)])
    twin = z + 1 - 2 * (z % 2)

    def slot(j, k):
        return k // 2 * (2 * nx) + 2 * j + k % 2

    def cols(q):
        return pl.ds(q * piece, piece)

    barrier = pltpu.get_barrier_semaphore()
    for j in range(1, n_ep):
        pl.semaphore_signal(barrier, inc=1, device_id=((me + j) % n_ep, tp), device_id_type=MESH)
    for j in range(1, n_tp):
        pl.semaphore_signal(barrier, inc=1, device_id=(me, (tp + j) % n_tp), device_id_type=MESH)
    load = pltpu.make_async_copy(tokens_ref, tok.at[pl.ds(0, tokens_ref.shape[0])], local_sem.at[2])
    load.start()


    def slot_rows(s):
        return pl.ds(s * rows if isinstance(s, int) else pl.multiple_of(s * rows, 16), rows)

    def tok_copy(from_slot, to_slot, h, target, send):
        part = pl.ds(edges[h], edges[h + 1] - edges[h])
        return pltpu.make_async_remote_copy(
            src_ref=tok.at[slot_rows(from_slot), part],
            dst_ref=tok.at[slot_rows(to_slot), part],
            send_sem=send, recv_sem=tok_recv.at[to_slot, h],
            device_id=target, device_id_type=MESH,
        )

    def tok_wait(s, h):
        tok_copy(s, s, h, (me, tp), tok_send.at[0, 0, 0]).wait_recv()

    def along(k, h, d):
        to = by_z([
            place_of[zz + d][near[zz][k]] if 0 <= zz + d < nz else 0 for zz in range(nz)
        ])
        return tok_copy(
            slot(0, k), slot(0, to), h, (me + d * nx, tp), tok_send.at[k, (1 - d) // 2, h]
        )

    def across(k, h, j):
        return tok_copy(
            slot(0, k), slot(nx - j, k), h, (z * nx + (x + j) % nx, tp), tok_send.at[k, 1 + j, h]
        )

    def onward(k, to, h):
        return tok_copy(
            slot(1, k), slot(1, to), h, (me + (twin - z) * nx, tp), hyb_send.at[h]
        )

    def crosses(k, h):
        if hyb and k == nz - 1 and h == parts - 1:
            return inner
        if hyb and k == nz - 2:
            return ends
        return lambda: True

    log = []

    def launch(conds, copy):
        log.append((conds, copy))
        when(conds, lambda: copy().start())

    def send_block(conds, k, h):
        bind = functools.partial
        for d in (1, -1):
            goes = [
                0 <= zz + d < nz and (near[zz][k] - zz) * d <= 0 for zz in range(nz)
            ]
            launch(conds + [lambda goes=goes: flag(goes)], bind(along, k, h, d))
        for j in range(1, nx):
            launch(conds + [crosses(k, h)], bind(across, k, h, j))

    def stage(step, h):
        for k in range(1, nz):
            here = [abs(near[zz][k] - zz) == step for zz in range(nz)]
            if any(here):
                cond = lambda here=here: flag(here)
                when([cond], lambda: tok_wait(slot(0, k), h))
                send_block([cond], k, h)
        if hyb and step == 1:
            tok_wait(slot(1, 0), h)
            launch([ends], functools.partial(onward, 0, nz - 2, h))
        if hyb and step == nz - 1 and h == parts - 1:
            when([inner], lambda: tok_wait(slot(1, nz - 1), h))
            launch([inner], functools.partial(onward, nz - 1, nz - 1, h))

    def cross_wait(half):
        for j in range(1, nx):
            for k in (2 * half, 2 * half + 1):
                for h in range(parts):
                    if hyb and k == 0:
                        continue
                    conds = [ends] if hyb and k == nz - 1 and h == parts - 1 else []
                    when(conds, lambda: tok_wait(slot(j, k), h))


    shared_at = pl.ds(0, extra)
    if s_gate_ref.shape[0] > extra:
        shared_at = pl.ds(pl.multiple_of(me * extra, extra), extra)

    def w_parts(k):
        slab = wall.at[tp]
        if k < pieces:
            at, r0 = pl.ds(k * pr, pr), 2 * extra + 2 * k * pr
            parts = [
                (gate_ref.at[at], slab.at[pl.ds(r0, pr)]),
                (up_ref.at[at], slab.at[pl.ds(r0 + pr, pr)]),
            ]
            if k == 0:
                parts += [
                    (s_gate_ref.at[shared_at], slab.at[pl.ds(0, extra)]),
                    (s_up_ref.at[shared_at], slab.at[pl.ds(extra, extra)]),
                ]
            return parts
        q = cols(k - pieces)
        return [
            (down_ref.at[:, q], slab.at[pl.ds(down_at, routed), q]),
            (s_down_ref.at[shared_at, q], slab.at[pl.ds(down_at + routed, extra), q]),
        ]

    def w_place(k, owner):
        if k == 0:
            return wall.at[owner, pl.ds(0, 2 * (extra + pr))]
        if k < pieces:
            return wall.at[owner, pl.ds(2 * (extra + k * pr), 2 * pr)]
        return wall.at[owner, pl.ds(down_at, routed + extra), cols(k - pieces)]

    def w_copy(k, by, way, refs=None):
        if way < 2:
            target = (me, tp + nc if way == 0 else tp - nc)
        else:
            target = (me, y * nc + (c + way - 1) % nc)
        owner = by * nc + c
        if refs is None:
            refs = (wall.at[owner],) * 2 if k is None else (w_place(k, owner),) * 2
        return pltpu.make_async_remote_copy(
            src_ref=refs[0], dst_ref=refs[1], send_sem=w_send.at[by, way],
            recv_sem=w_recv.at[0 if k is None else k, owner],
            device_id=target, device_id_type=MESH,
        )

    def w_wait(k, owner):
        pltpu.make_async_remote_copy(
            src_ref=w_place(k, owner), dst_ref=w_place(k, owner), send_sem=w_send.at[0, 0],
            recv_sem=w_recv.at[k, owner], device_id=(me, tp), device_id_type=MESH,
        ).wait_recv()

    def each_own(copy_of, act):
        pl.when(y < ny - 1)(lambda: act(copy_of(0)))
        pl.when(y > 0)(lambda: act(copy_of(1)))
        for way in range(2, 1 + nc):
            act(copy_of(way))

    def each_forward(copy_of, step, act, arrive):
        @pl.when(y >= step)
        def _():
            b = y - step
            arrive(b)
            pl.when(y < ny - 1)(lambda: act(copy_of(b, 0)))
            for way in range(2, 1 + nc):
                act(copy_of(b, way))

        @pl.when(y + step <= ny - 1)
        def _():
            b = y + step
            arrive(b)
            pl.when(y > 0)(lambda: act(copy_of(b, 1)))
            for way in range(2, 1 + nc):
                act(copy_of(b, way))

    start = lambda copy: copy.start()
    finish = lambda copy: copy.wait_send()

    def w_gathered(k):
        for step in range(1, ny):
            each_forward(
                lambda b, way: w_copy(k, b, way), step, start, lambda b: w_wait(k, b * nc + c)
            )

    def w_across(k):
        for j in range(1, nc):
            for by in range(ny):
                w_wait(k, by * nc + (c + j) % nc)


    def side_source(ref, to):
        if len(ref.shape) == 3:
            return ref.at[to]
        return ref.at[:, pl.ds(pl.multiple_of(to * side_cols, side_cols), side_cols)]

    def side_copy(j, p):
        to = (me + j) % n_ep
        return pltpu.make_async_remote_copy(
            src_ref=side_source((side_in_ref, side_out_ref)[p], to),
            dst_ref=side.at[p * n_ep + me],
            send_sem=side_send, recv_sem=side_recv, device_id=(to, tp), device_id_type=MESH,
        )

    def side_all():
        whole = side.at[pl.ds(0, n_ep - 1)]
        return pltpu.make_async_remote_copy(
            src_ref=whole, dst_ref=whole, send_sem=side_send, recv_sem=side_recv,
            device_id=(me, tp), device_id_type=MESH,
        )

    def side_own(p):
        return pltpu.make_async_copy(
            side_source((side_in_ref, side_out_ref)[p], me), side.at[p * n_ep + me],
            local_sem.at[1],
        )

    def swap_copy(half):
        part = side.at[pl.ds(half * n_ep, n_ep)]
        return pltpu.make_async_remote_copy(
            src_ref=part, dst_ref=part, send_sem=swap_send, recv_sem=swap_recv,
            device_id=(me, y * nc + 1 - c), device_id_type=MESH,
        )


    def aux_copy(k, j):
        to = by_z([near[zz][k] for zz in range(nz)]) * nx + (x + j) % nx
        k_there = by_z([place_of[near[zz][k]][zz] for zz in range(nz)])
        return pltpu.make_async_remote_copy(
            src_ref=saux.at[to], dst_ref=sc.at[slot((nx - j) % nx, k_there)],
            send_sem=aux_send, recv_sem=aux_recv, device_id=(to, tp), device_id_type=MESH,
        )

    def aux_all():
        return pltpu.make_async_remote_copy(
            src_ref=saux.at[pl.ds(0, n_ep - 1)], dst_ref=sc.at[pl.ds(0, n_ep - 1)],
            send_sem=aux_send, recv_sem=aux_recv, device_id=(me, tp), device_id_type=MESH,
        )

    for k in range(pieces + chunks):
        for part in w_parts(k):
            pltpu.make_async_copy(*part, local_sem.at[0]).start()
    for p in range(nc):
        pl.when(c == p)(lambda: side_own(p).start())

    load.wait()
    values = tok[slot_rows(0), :].astype(jnp.float32)
    scale_inv = lax.rsqrt(jnp.mean(values * values, axis=-1, keepdims=True) + norm_eps)
    normed = (values * scale_inv * gain_ref[...]).astype(jnp.bfloat16)
    tok[slot_rows(0), :] = normed

    pl.semaphore_wait(barrier, n_ep + n_tp - 2)
    for p in range(nc):
        def side_go(p=p):
            for j in range(1, n_ep):
                side_copy(j, p).start()

        pl.when(c == p)(side_go)
    for h in range(parts):
        send_block([], 0, h)
    for k in range(pieces + chunks):
        for refs in w_parts(k):
            each_own(lambda way: w_copy(k, y, way, refs), start)

    side_vector = side_gate_ref[...].astype(jnp.float32)
    lanes = side_vector.shape[1]
    side_vector = jnp.concatenate(
        [jnp.broadcast_to(side_vector[i : i + 1], (8, lanes)) for i in range(width // lanes)],
        axis=1,
    ).astype(jnp.bfloat16)
    opening = lax.dot_general(side_vector, normed, NT, preferred_element_type=jnp.float32)
    opening = 1.0 / (1.0 + jnp.exp(-opening))
    ids, route = ids_ref[...], route_ref[...]
    row = lax.broadcasted_iota(jnp.int32, (8, rows), 0)
    for to in range(n_ep):
        block = jnp.where(row == local_experts, opening, 0.0)
        for e in range(local_experts):
            hit = jnp.where(ids == to * local_experts + e, route, 0.0)
            block = jnp.where(row == e, jnp.sum(hit, axis=0, keepdims=True), block)
        gap = sc.shape[2] - rows
        saux[to] = jnp.concatenate([block, jnp.zeros((8, gap), jnp.float32)], axis=1)
    sc[0] = saux[me]
    for k in range(nz):
        for j in range(nx):
            if k or j:
                aux_copy(k, j).start()


    def tile_rows(t):
        return pl.ds(pl.multiple_of(t * tile, 16), tile)

    def column(at, n):
        picked = scol[at, :]
        lane = lax.broadcasted_iota(jnp.int32, picked.shape, 1)
        return jnp.sum(jnp.where(lane == n, picked, 0.0), axis=1, keepdims=True)

    def nt(a, b):
        return lax.dot_general(a, b, NT, preferred_element_type=jnp.float32)

    def unit(t, p):
        at = tile_rows(t)
        r0 = 2 * extra + p * (2 * pr)
        if not isinstance(p, int):
            r0 = pl.multiple_of(r0, 16)
        a = tok[at, :]
        gate = wall[:, pl.ds(r0, pr), :].reshape(piece_units, width)
        up = wall[:, pl.ds(r0 + pr, pr), :].reshape(piece_units, width)
        gated = silu(nt(a, gate)) * nt(a, up) * column(at, p // per_expert)
        to = p * piece_units if isinstance(p, int) else pl.multiple_of(p * piece_units, 128)
        hidden[at, pl.ds(to, piece_units)] = gated.astype(jnp.bfloat16)

    def units(t0, t1, p0, p1):
        n = p1 - p0
        if (t1 - t0) * n > 0:
            def step(i, carry):
                unit(t0 + i // n, p0 + i % n)
                return carry

            lax.fori_loop(0, (t1 - t0) * n, step, 0)

    def extras(t0, t1):
        def step(t, carry):
            at = tile_rows(t)
            a = tok[at, :]
            both = jnp.concatenate([
                wall[:, :extra, :].reshape(shared_units, width),
                wall[:, extra : 2 * extra, :].reshape(shared_units, width),
            ], axis=0)
            both = nt(a, both)
            gated = silu(both[:, :shared_units]) * both[:, shared_units:]
            hidden[at, pieces * piece_units :] = gated.astype(jnp.bfloat16)
            side_part = jnp.dot(
                a, side[:n_ep].reshape(width, side_cols), preferred_element_type=jnp.float32
            )
            side_hid[at] = (silu(side_part) * column(at, local_experts)).astype(jnp.bfloat16)
            return carry

        lax.fori_loop(t0, t1, step, 0)

    for h in range(parts):
        stage(1, h)
    pltpu.make_async_copy(wall.at[tp], wall.at[tp], local_sem.at[0]).wait()
    w_gathered(0)
    aux_all().wait_recv()
    for s in range(n_ep):
        scol[slot_rows(s), :] = sc[s].T[:rows]
    w_across(0)
    units(0, 1, 0, 1)
    for h in range(parts - 1):
        stage(2, h)
    w_gathered(1)
    stage(2, parts - 1)
    w_across(1)
    units(0, 1, 1, 2)
    cross_wait(0)
    units(1, nx, 0, 2)
    for s in range(3, nz):
        for h in range(parts - 1):
            stage(s, h)
    for p in range(2, pieces - 1):
        w_gathered(p)
    for p in range(nc):
        pl.when(c == p)(lambda: side_own(p).wait())
    side_all().wait_recv()
    swap_copy(c).start()
    for p in range(2, pieces - 1):
        w_across(p)
    units(0, nx, 2, pieces - 1)
    for s in range(3, nz):
        stage(s, parts - 1)
    units(nx, nx + 1, 0, pieces - 1)
    w_gathered(pieces - 1)
    swap_copy(1 - c).wait_recv()
    extras(0, nx + 1)
    w_across(pieces - 1)
    units(0, nx + 1, pieces - 1, pieces)
    w_gathered(pieces)
    for half in range(1, nz // 2):
        cross_wait(half)
    units(nx + 1, tiles, 0, pieces // 2)
    w_across(pieces)


    def x_index(j, k, q):
        return ((j - 1) * nz + k) * chunks + q

    def x_copy(q, j, k):
        i = x_index(j, k, q)
        return pltpu.make_async_remote_copy(
            src_ref=xs.at[i], dst_ref=xr.at[i], send_sem=x_send, recv_sem=x_recv.at[i],
            device_id=(z * nx + (x + j) % nx, tp), device_id_type=MESH,
        )

    def x_total(n):
        return pltpu.make_async_remote_copy(
            src_ref=xs.at[pl.ds(0, n)], dst_ref=xr.at[pl.ds(0, n)], send_sem=x_send,
            recv_sem=x_recv.at[0], device_id=(me, tp), device_id_type=MESH,
        )

    def h_copy(k, q):
        return pltpu.make_async_remote_copy(
            src_ref=xs.at[x_index(1, k, q)], dst_ref=hgot.at[q], send_sem=h_send,
            recv_sem=h_recv.at[q], device_id=(me + (twin - z) * nx, tp), device_id_type=MESH,
        )

    def h_total(n):
        return pltpu.make_async_remote_copy(
            src_ref=xs.at[pl.ds(0, n)], dst_ref=hgot.at[pl.ds(0, n)], send_sem=h_send,
            recv_sem=h_recv.at[0], device_id=(me, tp), device_id_type=MESH,
        )

    def z_copy(q, dz, right):
        return pltpu.make_async_remote_copy(
            src_ref=sent.at[dz * chunks + q], dst_ref=got.at[(dz + right) * chunks + q],
            send_sem=r_send if right else l_send, recv_sem=z_recv.at[(dz + right) * chunks + q],
            device_id=(me + nx if right else me - nx, tp), device_id_type=MESH,
        )

    def z_total(n, right):
        return pltpu.make_async_remote_copy(
            src_ref=sent.at[pl.ds(0, n)], dst_ref=got.at[pl.ds(0, n)],
            send_sem=r_send if right else l_send, recv_sem=z_recv.at[0],
            device_id=(me, tp), device_id_type=MESH,
        )

    blocks_per = piece // side_rows

    def product(q, j, half):
        down = jnp.concatenate(
            [
                wall[:, down_at + p * pr : down_at + (p + 1) * pr, cols(q)].reshape(
                    piece_units, piece
                )
                for p in range(pieces)
            ]
            + [wall[:, down_at + routed :, cols(q)].reshape(shared_units, piece)],
            axis=0,
        )
        side_down = side[pl.ds(n_ep + q * blocks_per, blocks_per)].reshape(piece, side_cols)
        at = tile_rows(half * nx + j)
        return jnp.dot(hidden[at], down, preferred_element_type=jnp.float32) + nt(
            side_hid[at], side_down
        )

    def detour(q, k):
        return hyb and k == 3 and q < chunks // 2

    def leave(q, j, k):
        go = lambda: x_copy(q, j, k).start()
        if detour(q, k):
            when([ends], lambda: h_copy(k, q).start())
        elif hyb and k == 2:
            when([ends], go)
        elif hyb and k == 0:
            when([inner], go)
        else:
            go()

    def partial_sum(q, half, j):
        value = product(q, j, half).astype(jnp.bfloat16)
        for i in (1, 0):
            k = 2 * half + i
            xs[x_index(j, k, q)] = value[i * rows : (i + 1) * rows]
            if q < chunks // 2 or k == nz - 1:
                leave(q, j, k)
            if hyb and k == 2:
                when([inner], lambda: h_copy(k, q).start())

    def own_sum(q, half):
        value = product(q, 0, half)
        for i in range(2):
            acc[(2 * half + i) * chunks + q] = value[i * rows : (i + 1) * rows]

    def relay(q):
        def pass_on(k):
            h_copy(k, q).wait_recv()
            i = x_index(1, k, q)
            value = xs[i].astype(jnp.float32) + hgot[q].astype(jnp.float32)
            xs[i] = value.astype(jnp.bfloat16)
            x_copy(q, 1, k).start()

        if hyb:
            when([ends], lambda: pass_on(0))
            if detour(q, 3):
                when([inner], lambda: pass_on(3))

    def fold(q, k):
        conds = []
        if detour(q, k):
            conds = [inner]
        if hyb and k == 2:
            conds = [ends]

        def add():
            value = acc[k * chunks + q]
            for j in range(1, nx):
                x_copy(q, j, k).wait_recv()
                value = value + xr[x_index(j, k, q)].astype(jnp.float32)
            acc[k * chunks + q] = value

        when(conds, add)

    def move_on(q, k):
        fold(q, k)
        dz = by_z([near[zz][k] for zz in range(nz)])

        def move(right, far):
            def act():
                value = acc[k * chunks + q]
                mine = dz * chunks + q

                @pl.when(z == far)
                def _():
                    sent[mine] = value.astype(jnp.bfloat16)

                @pl.when(z != far)
                def _():
                    z_copy(q, dz, right).wait_recv()
                    more = got[(dz + right) * chunks + q].astype(jnp.float32)
                    sent[mine] = (value + more).astype(jnp.bfloat16)

                z_copy(q, dz, right).start()

            return act

        when([lambda: flag([near[zz][k] > zz for zz in range(nz)])], move(1, 0))
        when([lambda: flag([near[zz][k] < zz for zz in range(nz)])], move(0, nz - 1))

    def settle(q):
        fold(q, 0)

        @pl.when(z > 0)
        def _():
            z_copy(q, z, 1).wait_recv()
            acc[q] += got[(z + 1) * chunks + q].astype(jnp.float32)

        @pl.when(z < nz - 1)
        def _():
            z_copy(q, z, 0).wait_recv()
            acc[q] += got[z * chunks + q].astype(jnp.float32)

        out_v[:, cols(q)] = acc[q].astype(jnp.bfloat16)
        pltpu.make_async_copy(out_v.at[:, cols(q)], out_ref.at[:, cols(q)], local_sem.at[2]).start()

    halves = nz // 2
    first = chunks // 2
    late = range(first, chunks)

    def own_sums(q):
        for half in reversed(range(halves)):
            own_sum(q, half)
            if half and detour(q, nz - 1):
                when([ends], lambda: move_on(q, nz - 1))

    def early(q):
        for j in range(1, nx):
            partial_sum(q, 0, j)
        own_sums(q)

    def rest(q):
        for half in reversed(range(1, halves)):
            for j in range(1, nx):
                partial_sum(q, half, j)

    def sums(q):
        w_across(pieces + q)
        rest(q)
        early(q)

    def move_all(q):
        if not detour(q, nz - 1):
            for k in range(nz - 1, 0, -1):
                move_on(q, k)
            return
        when([inner], lambda: move_on(q, 3))
        for k in (2, 1):
            when([ends], lambda: move_on(q, k))
            when([inner], lambda: move_on(q, 3 - k))

    gather = lambda q: w_gathered(pieces + q)
    early(0)
    gather(1)
    units(nx + 1, tiles, pieces // 2, pieces)
    w_across(pieces + 1)
    early(1)
    extras(nx + 1, tiles)
    gather(2)
    rest(0)
    rest(1)
    relay(0)
    gather(3)
    sums(2)
    relay(1)
    sums(3)
    relay(2)
    gather(4)
    move_all(0)
    sums(4)
    gather(5)
    relay(3)
    move_all(1)
    gather(6)
    sums(5)
    sums(6)
    gather(7)
    move_all(2)
    sums(7)
    for k in range(nz - 2, -1, -1):
        for q in late:
            for j in range(1, nx):
                leave(q, j, k)
            if k == 0:
                relay(q)
    for q in range(3, first):
        move_all(q)
    for k in range(nz - 1, 0, -1):
        for q in late:
            move_on(q, k)
        if k == nz - 1:
            settle(0)
            settle(1)
        elif k == nz - 2:
            for q in range(2, first):
                settle(q)
    for q in late:
        settle(q)

    for conds, copy in log:
        when(conds, lambda: copy().wait_send())
    pltpu.make_async_copy(out_v, out_ref, local_sem.at[2]).wait()
    each_own(lambda way: w_copy(None, y, way), finish)
    for step in range(1, ny):
        each_forward(lambda b, way: w_copy(None, b, way), step, finish, lambda b: None)
    side_all().wait_send()
    swap_copy(c).wait_send()
    aux_all().wait_send()
    count = (nx - 1) * nz * chunks
    if hyb:
        when([ends], lambda: x_total(count - chunks // 2).wait_send())
        when([inner], lambda: x_total(count - chunks).wait_send())
        when([ends], lambda: h_total(chunks // 2).wait_send())
        when([inner], lambda: h_total(chunks).wait_send())
    else:
        x_total(count).wait_send()
    for zz in range(nz):
        if zz < nz - 1:
            pl.when(z == zz)(lambda: z_total((nz - 1 - zz) * chunks, 1).wait_send())
        if zz > 0:
            pl.when(z == zz)(lambda: z_total(zz * chunks, 0).wait_send())


def body(
    nx,
    nc,
    tokens,
    norm_gain,
    expert_ids,
    route_weights,
    expert_gate,
    expert_up,
    expert_down,
    shared_gate,
    shared_up,
    shared_down,
    side_in,
    side_out,
    side_gate,
):
    tok_count, width = tokens.shape
    n_ep, n_tp = lax.axis_size("ep"), lax.axis_size("tp")
    nz, ny = n_ep // nx, n_tp // nc
    me = lax.axis_index("ep")
    local_experts, ff_part, _ = expert_gate.shape
    routed = local_experts * ff_part
    shared_rows = shared_gate.shape[0] // n_ep
    side_rows, side_all = side_in.shape
    side_cols = side_all // n_ep
    chunks = 8
    pieces = 2 * local_experts
    piece = width // chunks
    extra = -(-shared_rows // 16) * 16
    padded = -(-tok_count // 128) * 128

    def shared_part(array):
        if shared_rows % 16 == 0:
            return array
        own = lax.dynamic_slice_in_dim(array, me * shared_rows, shared_rows, 0)
        return jnp.pad(own, ((0, extra - shared_rows), (0, 0)))

    def side_part(array):
        if side_cols % 128 == 0:
            return array
        return array.reshape(side_rows, n_ep, side_cols).transpose(1, 0, 2)

    bf16, f32 = jnp.bfloat16, jnp.float32
    dma = pltpu.SemaphoreType.DMA
    dims = (nz, nx, ny, nc, local_experts, pieces, extra, chunks)
    return pl.pallas_call(
        functools.partial(kernel, dims),
        out_shape=jax.ShapeDtypeStruct((tok_count, width), bf16),
        in_specs=[pl.BlockSpec(memory_space=pl.ANY)]
        + [pl.BlockSpec(memory_space=pltpu.VMEM)] * 4
        + [pl.BlockSpec(memory_space=pl.ANY)] * 8,
        out_specs=pl.BlockSpec(memory_space=pl.ANY),
        scratch_shapes=[
            pltpu.VMEM((n_ep * tok_count, width), bf16),
            pltpu.VMEM((n_tp, 3 * (routed + extra), width), bf16),
            pltpu.VMEM((2 * n_ep, side_rows, side_cols), bf16),
            pltpu.VMEM((n_ep * tok_count, n_tp * (routed + extra)), bf16),
            pltpu.VMEM((n_ep * tok_count, side_cols), bf16),
            pltpu.VMEM((nz * chunks, tok_count, piece), f32),
            pltpu.VMEM(((nx - 1) * nz * chunks, tok_count, piece), bf16),
            pltpu.VMEM(((nx - 1) * nz * chunks, tok_count, piece), bf16),
            pltpu.VMEM((nz * chunks, tok_count, piece), bf16),
            pltpu.VMEM(((nz + 1) * chunks, tok_count, piece), bf16),
            pltpu.VMEM((chunks if nx == 2 else 1, tok_count, piece), bf16),
            pltpu.VMEM((n_ep, 8, padded), f32),
            pltpu.VMEM((n_ep, 8, padded), f32),
            pltpu.VMEM((n_ep * tok_count, 8), f32),
            pltpu.VMEM((tok_count, width), bf16),
            dma((nz, 1 + nx, 3)),
            dma((n_ep, 3)),
            dma((3,)),
            dma((ny, 1 + nc)),
            dma((pieces + chunks, n_tp)),
            dma,
            dma,
            dma,
            dma,
            dma((3,)),
            dma,
            dma,
            dma,
            dma(((nx - 1) * nz * chunks,)),
            dma,
            dma,
            dma(((nz + 1) * chunks,)),
            dma,
            dma((chunks,)),
        ],
        compiler_params=pltpu.CompilerParams(
            collective_id=0, has_side_effects=True, vmem_limit_bytes=63000 * 1024
        ),
        name="layer",
    )(
        tokens, norm_gain[None, :], expert_ids.T, route_weights.T, side_gate.reshape(-1, 128),
        expert_gate.reshape(routed, width), expert_up.reshape(routed, width),
        expert_down.reshape(routed, width), shared_part(shared_gate), shared_part(shared_up),
        shared_part(shared_down), side_part(side_in), side_part(side_out),
    )


def solution(mesh):
    devices = mesh.devices
    nx = len({d.coords[0] for d in devices[:, 0]})
    nc = len({d.core_on_chip for d in devices[0, :]})
    placed = (
        P(("ep", "tp"), None),
        P(),
        P(("ep", "tp"), None),
        P(("ep", "tp"), None),
        P("ep", "tp", None),
        P("ep", "tp", None),
        P("ep", "tp", None),
        P("tp", None),
        P("tp", None),
        P("tp", None),
        P("ep", None),
        P("ep", None),
        P(),
    )
    return jax.shard_map(
        functools.partial(body, nx, nc),
        mesh=mesh,
        in_specs=placed,
        out_specs=P(("ep", "tp"), None),
        check_vma=False,
    )
```

```python
import functools

import jax
import jax.numpy as jnp
from jax import lax
from jax.experimental import pallas as pl
from jax.experimental.pallas import tpu as pltpu
from jax.sharding import PartitionSpec as P

norm_eps = 1.0
MESH = pl.DeviceIdType.MESH
NT = (((1,), (1,)), ((), ()))


def silu(v):
    return v / (1.0 + jnp.exp(-v))


def when(conds, act):
    conds = [cond() for cond in conds]
    if any(cond is False for cond in conds):
        return
    conds = [cond for cond in conds if cond is not True]
    if not conds:
        act()
        return
    both = conds[0]
    for cond in conds[1:]:
        both = jnp.logical_and(both, cond)
    pl.when(both)(act)


def kernel(
    dims,
    tokens_ref, gain_ref, ids_ref, route_ref, side_gate_ref,
    gate_ref, up_ref, down_ref, s_gate_ref, s_up_ref, s_down_ref, side_in_ref, side_out_ref,
    out_ref,
    tok, wall, side, hidden, side_hid, acc, xs, xr, sent, got, hgot, saux, sc, scol, out_v,
    tok_send, tok_recv, hyb_send, know, w_send, w_recv, side_send, side_recv, swap_send, swap_recv,
    local_sem, aux_send, aux_recv, x_send, x_recv, r_send, l_send, z_recv, h_send, h_recv,
):
    nz, nx, ny, nc, local_experts, pieces, extra, chunks = dims
    n_ep, n_tp = nz * nx, ny * nc
    me, tp = lax.axis_index("ep"), lax.axis_index("tp")
    z, x = me // nx, me % nx
    y, c = tp // nc, tp % nc
    rows, width = tokens_ref.shape
    routed = gate_ref.shape[0]
    pr = routed // pieces
    per_expert = pieces // local_experts
    piece_units, shared_units = n_tp * pr, n_tp * extra
    side_rows, side_cols = side.shape[1:]
    piece = width // chunks
    unit_w = width // 16
    edges = [0, 5 * unit_w, 10 * unit_w, width]
    parts = len(edges) - 1
    down_at = 2 * (routed + extra)
    tile = 2 * rows
    hyb = nx == 2 and nz == 4
    tiles = n_ep // 2

    near = [
        sorted(range(nz), key=lambda b: (abs(b - zz), -b if 2 * zz < nz else b))
        for zz in range(nz)
    ]
    place_of = [[near[zz].index(b) for b in range(nz)] for zz in range(nz)]

    def by_z(values):
        out = values[0]
        if all(v == out for v in values):
            return out
        for zz in range(1, nz):
            out = jnp.where(z == zz, values[zz], out)
        return out

    def flag(values):
        values = [bool(v) for v in values]
        if all(values) or not any(values):
            return values[0]
        return by_z([int(v) for v in values]) == 1

    ends = lambda: flag([zz in (0, nz - 1) for zz in range(nz)])
    inner = lambda: flag([zz not in (0, nz - 1) for zz in range(nz)])
    twin = z + 1 - 2 * (z % 2)

    def slot(j, k):
        return k // 2 * (2 * nx) + 2 * j + k % 2

    def cols(q):
        return pl.ds(q * piece, piece)

    barrier = pltpu.get_barrier_semaphore()

    def tell(sem, ep, other):
        pl.semaphore_signal(sem, inc=1, device_id=(ep, other), device_id_type=MESH)

    def tell_near(sem):
        pl.when(z < nz - 1)(lambda: tell(sem, me + nx, tp))
        pl.when(z > 0)(lambda: tell(sem, me - nx, tp))
        for j in range(1, nx):
            tell(sem, z * nx + (x + j) % nx, tp)

    near_count = by_z([(zz > 0) + (zz < nz - 1) for zz in range(nz)]) + nx - 1
    tp_count = jnp.where(y > 0, 1, 0) + jnp.where(y < ny - 1, 1, 0) + nc - 1
    tell_near(barrier)
    pl.when(y < ny - 1)(lambda: tell(barrier, me, tp + nc))
    pl.when(y > 0)(lambda: tell(barrier, me, tp - nc))
    for j in range(1, nc):
        tell(barrier, me, y * nc + (c + j) % nc)
    load = pltpu.make_async_copy(tokens_ref, tok.at[pl.ds(0, tokens_ref.shape[0])], local_sem.at[2])
    load.start()


    def slot_rows(s):
        return pl.ds(s * rows if isinstance(s, int) else pl.multiple_of(s * rows, 16), rows)

    def tok_copy(from_slot, to_slot, h, target, send):
        part = pl.ds(edges[h], edges[h + 1] - edges[h])
        return pltpu.make_async_remote_copy(
            src_ref=tok.at[slot_rows(from_slot), part],
            dst_ref=tok.at[slot_rows(to_slot), part],
            send_sem=send, recv_sem=tok_recv.at[to_slot, h],
            device_id=target, device_id_type=MESH,
        )

    def tok_wait(s, h):
        tok_copy(s, s, h, (me, tp), tok_send.at[0, 0, 0]).wait_recv()

    def along(k, h, d):
        to = by_z([
            place_of[zz + d][near[zz][k]] if 0 <= zz + d < nz else 0 for zz in range(nz)
        ])
        return tok_copy(
            slot(0, k), slot(0, to), h, (me + d * nx, tp), tok_send.at[k, (1 - d) // 2, h]
        )

    def across(k, h, j):
        return tok_copy(
            slot(0, k), slot(nx - j, k), h, (z * nx + (x + j) % nx, tp), tok_send.at[k, 1 + j, h]
        )

    def onward(k, to, h):
        return tok_copy(
            slot(1, k), slot(1, to), h, (me + (twin - z) * nx, tp), hyb_send.at[h]
        )

    def crosses(k, h):
        if hyb and k == nz - 1 and h == parts - 1:
            return inner
        if hyb and k == nz - 2:
            return ends
        return lambda: True

    log = []

    def launch(conds, copy):
        log.append((conds, copy))
        when(conds, lambda: copy().start())

    def send_block(conds, k, h):
        bind = functools.partial
        for d in (1, -1):
            goes = [
                0 <= zz + d < nz and (near[zz][k] - zz) * d <= 0 for zz in range(nz)
            ]
            launch(conds + [lambda goes=goes: flag(goes)], bind(along, k, h, d))
        for j in range(1, nx):
            launch(conds + [crosses(k, h)], bind(across, k, h, j))

    def stage(step, h):
        for k in range(1, nz):
            here = [abs(near[zz][k] - zz) == step for zz in range(nz)]
            if any(here):
                cond = lambda here=here: flag(here)
                when([cond], lambda: tok_wait(slot(0, k), h))
                send_block([cond], k, h)
        if hyb and step == 1:
            tok_wait(slot(1, 0), h)
            launch([ends], functools.partial(onward, 0, nz - 2, h))
        if hyb and step == nz - 1 and h == parts - 1:
            when([inner], lambda: tok_wait(slot(1, nz - 1), h))
            launch([inner], functools.partial(onward, nz - 1, nz - 1, h))

    def cross_wait(half):
        for j in range(1, nx):
            for k in (2 * half, 2 * half + 1):
                for h in range(parts):
                    if hyb and k == 0:
                        continue
                    conds = [ends] if hyb and k == nz - 1 and h == parts - 1 else []
                    when(conds, lambda: tok_wait(slot(j, k), h))


    shared_at = pl.ds(0, extra)
    if s_gate_ref.shape[0] > extra:
        shared_at = pl.ds(pl.multiple_of(me * extra, extra), extra)

    def w_parts(k):
        slab = wall.at[tp]
        if k < pieces:
            at, r0 = pl.ds(k * pr, pr), 2 * extra + 2 * k * pr
            parts = [
                (gate_ref.at[at], slab.at[pl.ds(r0, pr)]),
                (up_ref.at[at], slab.at[pl.ds(r0 + pr, pr)]),
            ]
            if k == 0:
                parts += [
                    (s_gate_ref.at[shared_at], slab.at[pl.ds(0, extra)]),
                    (s_up_ref.at[shared_at], slab.at[pl.ds(extra, extra)]),
                ]
            return parts
        q = cols(k - pieces)
        return [
            (down_ref.at[:, q], slab.at[pl.ds(down_at, routed), q]),
            (s_down_ref.at[shared_at, q], slab.at[pl.ds(down_at + routed, extra), q]),
        ]

    def w_place(k, owner):
        if k == 0:
            return wall.at[owner, pl.ds(0, 2 * (extra + pr))]
        if k < pieces:
            return wall.at[owner, pl.ds(2 * (extra + k * pr), 2 * pr)]
        return wall.at[owner, pl.ds(down_at, routed + extra), cols(k - pieces)]

    def w_copy(k, by, way, refs=None):
        if way < 2:
            target = (me, tp + nc if way == 0 else tp - nc)
        else:
            target = (me, y * nc + (c + way - 1) % nc)
        owner = by * nc + c
        if refs is None:
            refs = (wall.at[owner],) * 2 if k is None else (w_place(k, owner),) * 2
        return pltpu.make_async_remote_copy(
            src_ref=refs[0], dst_ref=refs[1], send_sem=w_send.at[by, way],
            recv_sem=w_recv.at[0 if k is None else k, owner],
            device_id=target, device_id_type=MESH,
        )

    def w_wait(k, owner):
        pltpu.make_async_remote_copy(
            src_ref=w_place(k, owner), dst_ref=w_place(k, owner), send_sem=w_send.at[0, 0],
            recv_sem=w_recv.at[k, owner], device_id=(me, tp), device_id_type=MESH,
        ).wait_recv()

    def each_own(copy_of, act):
        pl.when(y < ny - 1)(lambda: act(copy_of(0)))
        pl.when(y > 0)(lambda: act(copy_of(1)))
        for way in range(2, 1 + nc):
            act(copy_of(way))

    def each_forward(copy_of, step, act, arrive):
        @pl.when(y >= step)
        def _():
            b = y - step
            arrive(b)
            pl.when(y < ny - 1)(lambda: act(copy_of(b, 0)))
            for way in range(2, 1 + nc):
                act(copy_of(b, way))

        @pl.when(y + step <= ny - 1)
        def _():
            b = y + step
            arrive(b)
            pl.when(y > 0)(lambda: act(copy_of(b, 1)))
            for way in range(2, 1 + nc):
                act(copy_of(b, way))

    start = lambda copy: copy.start()
    finish = lambda copy: copy.wait_send()

    def w_gathered(k):
        for step in range(1, ny):
            each_forward(
                lambda b, way: w_copy(k, b, way), step, start, lambda b: w_wait(k, b * nc + c)
            )

    def w_across(k):
        for j in range(1, nc):
            for by in range(ny):
                w_wait(k, by * nc + (c + j) % nc)


    def side_source(ref, to):
        if len(ref.shape) == 3:
            return ref.at[to]
        return ref.at[:, pl.ds(pl.multiple_of(to * side_cols, side_cols), side_cols)]

    def side_copy(j, p):
        to = (me + j) % n_ep
        return pltpu.make_async_remote_copy(
            src_ref=side_source((side_in_ref, side_out_ref)[p], to),
            dst_ref=side.at[p * n_ep + me],
            send_sem=side_send, recv_sem=side_recv, device_id=(to, tp), device_id_type=MESH,
        )

    def side_all():
        whole = side.at[pl.ds(0, n_ep - 1)]
        return pltpu.make_async_remote_copy(
            src_ref=whole, dst_ref=whole, send_sem=side_send, recv_sem=side_recv,
            device_id=(me, tp), device_id_type=MESH,
        )

    def side_own(p):
        return pltpu.make_async_copy(
            side_source((side_in_ref, side_out_ref)[p], me), side.at[p * n_ep + me],
            local_sem.at[1],
        )

    def swap_copy(half):
        part = side.at[pl.ds(half * n_ep, n_ep)]
        return pltpu.make_async_remote_copy(
            src_ref=part, dst_ref=part, send_sem=swap_send, recv_sem=swap_recv,
            device_id=(me, y * nc + 1 - c), device_id_type=MESH,
        )


    def aux_copy(k, j):
        to = by_z([near[zz][k] for zz in range(nz)]) * nx + (x + j) % nx
        k_there = by_z([place_of[near[zz][k]][zz] for zz in range(nz)])
        return pltpu.make_async_remote_copy(
            src_ref=saux.at[to], dst_ref=sc.at[slot((nx - j) % nx, k_there)],
            send_sem=aux_send, recv_sem=aux_recv, device_id=(to, tp), device_id_type=MESH,
        )

    def aux_all():
        return pltpu.make_async_remote_copy(
            src_ref=saux.at[pl.ds(0, n_ep - 1)], dst_ref=sc.at[pl.ds(0, n_ep - 1)],
            send_sem=aux_send, recv_sem=aux_recv, device_id=(me, tp), device_id_type=MESH,
        )

    for k in range(pieces + chunks):
        for part in w_parts(k):
            pltpu.make_async_copy(*part, local_sem.at[0]).start()
    for p in range(nc):
        pl.when(c == p)(lambda: side_own(p).start())

    load.wait()
    values = tok[slot_rows(0), :].astype(jnp.float32)
    scale_inv = lax.rsqrt(jnp.mean(values * values, axis=-1, keepdims=True) + norm_eps)
    normed = (values * scale_inv * gain_ref[...]).astype(jnp.bfloat16)
    tok[slot_rows(0), :] = normed

    pl.semaphore_wait(barrier, near_count + tp_count)
    for h in range(parts):
        send_block([], 0, h)
    tell_near(know.at[0])
    for k in range(pieces + chunks):
        for refs in w_parts(k):
            each_own(lambda way: w_copy(k, y, way, refs), start)

    for i in range(1, nz - 1):
        pl.semaphore_wait(know.at[i - 1], near_count)
        tell_near(know.at[i])
    side_vector = side_gate_ref[...].astype(jnp.float32)
    lanes = side_vector.shape[1]
    side_vector = jnp.concatenate(
        [jnp.broadcast_to(side_vector[i : i + 1], (8, lanes)) for i in range(width // lanes)],
        axis=1,
    ).astype(jnp.bfloat16)
    opening = lax.dot_general(side_vector, normed, NT, preferred_element_type=jnp.float32)
    opening = 1.0 / (1.0 + jnp.exp(-opening))
    ids, route = ids_ref[...], route_ref[...]
    row = lax.broadcasted_iota(jnp.int32, (8, rows), 0)
    for to in range(n_ep):
        block = jnp.where(row == local_experts, opening, 0.0)
        for e in range(local_experts):
            hit = jnp.where(ids == to * local_experts + e, route, 0.0)
            block = jnp.where(row == e, jnp.sum(hit, axis=0, keepdims=True), block)
        gap = sc.shape[2] - rows
        saux[to] = jnp.concatenate([block, jnp.zeros((8, gap), jnp.float32)], axis=1)
    sc[0] = saux[me]
    pl.semaphore_wait(know.at[nz - 2], near_count)
    for p in range(nc):
        def side_go(p=p):
            for j in range(1, n_ep):
                side_copy(j, p).start()

        pl.when(c == p)(side_go)
    for k in range(nz):
        for j in range(nx):
            if k or j:
                aux_copy(k, j).start()


    def tile_rows(t):
        return pl.ds(pl.multiple_of(t * tile, 16), tile)

    def column(at, n):
        picked = scol[at, :]
        lane = lax.broadcasted_iota(jnp.int32, picked.shape, 1)
        return jnp.sum(jnp.where(lane == n, picked, 0.0), axis=1, keepdims=True)

    def nt(a, b):
        return lax.dot_general(a, b, NT, preferred_element_type=jnp.float32)

    def unit(t, p):
        at = tile_rows(t)
        r0 = 2 * extra + p * (2 * pr)
        if not isinstance(p, int):
            r0 = pl.multiple_of(r0, 16)
        a = tok[at, :]
        gate = wall[:, pl.ds(r0, pr), :].reshape(piece_units, width)
        up = wall[:, pl.ds(r0 + pr, pr), :].reshape(piece_units, width)
        gated = silu(nt(a, gate)) * nt(a, up) * column(at, p // per_expert)
        to = p * piece_units if isinstance(p, int) else pl.multiple_of(p * piece_units, 128)
        hidden[at, pl.ds(to, piece_units)] = gated.astype(jnp.bfloat16)

    def units(t0, t1, p0, p1):
        n = p1 - p0
        if (t1 - t0) * n > 0:
            def step(i, carry):
                unit(t0 + i // n, p0 + i % n)
                return carry

            lax.fori_loop(0, (t1 - t0) * n, step, 0)

    def extras(t0, t1):
        def step(t, carry):
            at = tile_rows(t)
            a = tok[at, :]
            both = jnp.concatenate([
                wall[:, :extra, :].reshape(shared_units, width),
                wall[:, extra : 2 * extra, :].reshape(shared_units, width),
            ], axis=0)
            both = nt(a, both)
            gated = silu(both[:, :shared_units]) * both[:, shared_units:]
            hidden[at, pieces * piece_units :] = gated.astype(jnp.bfloat16)
            side_part = jnp.dot(
                a, side[:n_ep].reshape(width, side_cols), preferred_element_type=jnp.float32
            )
            side_hid[at] = (silu(side_part) * column(at, local_experts)).astype(jnp.bfloat16)
            return carry

        lax.fori_loop(t0, t1, step, 0)

    for h in range(parts):
        stage(1, h)
    pltpu.make_async_copy(wall.at[tp], wall.at[tp], local_sem.at[0]).wait()
    w_gathered(0)
    aux_all().wait_recv()
    for s in range(n_ep):
        scol[slot_rows(s), :] = sc[s].T[:rows]
    w_across(0)
    units(0, 1, 0, 1)
    for h in range(parts - 1):
        stage(2, h)
    w_gathered(1)
    stage(2, parts - 1)
    w_across(1)
    units(0, 1, 1, 2)
    cross_wait(0)
    units(1, nx, 0, 2)
    for s in range(3, nz):
        for h in range(parts - 1):
            stage(s, h)
    for p in range(2, pieces - 1):
        w_gathered(p)
    for p in range(nc):
        pl.when(c == p)(lambda: side_own(p).wait())
    side_all().wait_recv()
    swap_copy(c).start()
    for p in range(2, pieces - 1):
        w_across(p)
    units(0, nx, 2, pieces - 1)
    for s in range(3, nz):
        stage(s, parts - 1)
    units(nx, nx + 1, 0, pieces - 1)
    w_gathered(pieces - 1)
    swap_copy(1 - c).wait_recv()
    extras(0, nx + 1)
    w_across(pieces - 1)
    units(0, nx + 1, pieces - 1, pieces)
    w_gathered(pieces)
    for half in range(1, nz // 2):
        cross_wait(half)
    units(nx + 1, tiles, 0, pieces // 2)
    w_across(pieces)


    def x_index(j, k, q):
        return ((j - 1) * nz + k) * chunks + q

    def x_copy(q, j, k):
        i = x_index(j, k, q)
        return pltpu.make_async_remote_copy(
            src_ref=xs.at[i], dst_ref=xr.at[i], send_sem=x_send, recv_sem=x_recv.at[i],
            device_id=(z * nx + (x + j) % nx, tp), device_id_type=MESH,
        )

    def x_total(n):
        return pltpu.make_async_remote_copy(
            src_ref=xs.at[pl.ds(0, n)], dst_ref=xr.at[pl.ds(0, n)], send_sem=x_send,
            recv_sem=x_recv.at[0], device_id=(me, tp), device_id_type=MESH,
        )

    def h_copy(k, q):
        return pltpu.make_async_remote_copy(
            src_ref=xs.at[x_index(1, k, q)], dst_ref=hgot.at[q], send_sem=h_send,
            recv_sem=h_recv.at[q], device_id=(me + (twin - z) * nx, tp), device_id_type=MESH,
        )

    def h_total(n):
        return pltpu.make_async_remote_copy(
            src_ref=xs.at[pl.ds(0, n)], dst_ref=hgot.at[pl.ds(0, n)], send_sem=h_send,
            recv_sem=h_recv.at[0], device_id=(me, tp), device_id_type=MESH,
        )

    def z_copy(q, dz, right):
        return pltpu.make_async_remote_copy(
            src_ref=sent.at[dz * chunks + q], dst_ref=got.at[(dz + right) * chunks + q],
            send_sem=r_send if right else l_send, recv_sem=z_recv.at[(dz + right) * chunks + q],
            device_id=(me + nx if right else me - nx, tp), device_id_type=MESH,
        )

    def z_total(n, right):
        return pltpu.make_async_remote_copy(
            src_ref=sent.at[pl.ds(0, n)], dst_ref=got.at[pl.ds(0, n)],
            send_sem=r_send if right else l_send, recv_sem=z_recv.at[0],
            device_id=(me, tp), device_id_type=MESH,
        )

    blocks_per = piece // side_rows

    def product(q, j, half):
        down = jnp.concatenate(
            [
                wall[:, down_at + p * pr : down_at + (p + 1) * pr, cols(q)].reshape(
                    piece_units, piece
                )
                for p in range(pieces)
            ]
            + [wall[:, down_at + routed :, cols(q)].reshape(shared_units, piece)],
            axis=0,
        )
        side_down = side[pl.ds(n_ep + q * blocks_per, blocks_per)].reshape(piece, side_cols)
        at = tile_rows(half * nx + j)
        return jnp.dot(hidden[at], down, preferred_element_type=jnp.float32) + nt(
            side_hid[at], side_down
        )

    def detour(q, k):
        return hyb and k == 3 and q < chunks // 2

    def leave(q, j, k):
        go = lambda: x_copy(q, j, k).start()
        if detour(q, k):
            when([ends], lambda: h_copy(k, q).start())
        elif hyb and k == 2:
            when([ends], go)
        elif hyb and k == 0:
            when([inner], go)
        else:
            go()

    def partial_sum(q, half, j):
        value = product(q, j, half).astype(jnp.bfloat16)
        for i in (1, 0):
            k = 2 * half + i
            xs[x_index(j, k, q)] = value[i * rows : (i + 1) * rows]
            if q < chunks // 2 or k == nz - 1:
                leave(q, j, k)
            if hyb and k == 2:
                when([inner], lambda: h_copy(k, q).start())

    def own_sum(q, half):
        value = product(q, 0, half)
        for i in range(2):
            acc[(2 * half + i) * chunks + q] = value[i * rows : (i + 1) * rows]

    def relay(q):
        def pass_on(k):
            h_copy(k, q).wait_recv()
            i = x_index(1, k, q)
            value = xs[i].astype(jnp.float32) + hgot[q].astype(jnp.float32)
            xs[i] = value.astype(jnp.bfloat16)
            x_copy(q, 1, k).start()

        if hyb:
            when([ends], lambda: pass_on(0))
            if detour(q, 3):
                when([inner], lambda: pass_on(3))

    def fold(q, k):
        conds = []
        if detour(q, k):
            conds = [inner]
        if hyb and k == 2:
            conds = [ends]

        def add():
            value = acc[k * chunks + q]
            for j in range(1, nx):
                x_copy(q, j, k).wait_recv()
                value = value + xr[x_index(j, k, q)].astype(jnp.float32)
            acc[k * chunks + q] = value

        when(conds, add)

    def move_on(q, k):
        fold(q, k)
        dz = by_z([near[zz][k] for zz in range(nz)])

        def move(right, far):
            def act():
                value = acc[k * chunks + q]
                mine = dz * chunks + q

                @pl.when(z == far)
                def _():
                    sent[mine] = value.astype(jnp.bfloat16)

                @pl.when(z != far)
                def _():
                    z_copy(q, dz, right).wait_recv()
                    more = got[(dz + right) * chunks + q].astype(jnp.float32)
                    sent[mine] = (value + more).astype(jnp.bfloat16)

                z_copy(q, dz, right).start()

            return act

        when([lambda: flag([near[zz][k] > zz for zz in range(nz)])], move(1, 0))
        when([lambda: flag([near[zz][k] < zz for zz in range(nz)])], move(0, nz - 1))

    def settle(q):
        fold(q, 0)

        @pl.when(z > 0)
        def _():
            z_copy(q, z, 1).wait_recv()
            acc[q] += got[(z + 1) * chunks + q].astype(jnp.float32)

        @pl.when(z < nz - 1)
        def _():
            z_copy(q, z, 0).wait_recv()
            acc[q] += got[z * chunks + q].astype(jnp.float32)

        out_v[:, cols(q)] = acc[q].astype(jnp.bfloat16)
        pltpu.make_async_copy(out_v.at[:, cols(q)], out_ref.at[:, cols(q)], local_sem.at[2]).start()

    halves = nz // 2
    first = chunks // 2
    late = range(first, chunks)

    def own_sums(q):
        for half in reversed(range(halves)):
            own_sum(q, half)
            if half and detour(q, nz - 1):
                when([ends], lambda: move_on(q, nz - 1))

    def early(q):
        for j in range(1, nx):
            partial_sum(q, 0, j)
        own_sums(q)

    def rest(q):
        for half in reversed(range(1, halves)):
            for j in range(1, nx):
                partial_sum(q, half, j)

    def sums(q):
        w_across(pieces + q)
        rest(q)
        early(q)

    def move_all(q):
        if not detour(q, nz - 1):
            for k in range(nz - 1, 0, -1):
                move_on(q, k)
            return
        when([inner], lambda: move_on(q, 3))
        for k in (2, 1):
            when([ends], lambda: move_on(q, k))
            when([inner], lambda: move_on(q, 3 - k))

    gather = lambda q: w_gathered(pieces + q)
    early(0)
    gather(1)
    units(nx + 1, tiles, pieces // 2, pieces)
    w_across(pieces + 1)
    early(1)
    extras(nx + 1, tiles)
    gather(2)
    rest(0)
    rest(1)
    relay(0)
    gather(3)
    sums(2)
    relay(1)
    sums(3)
    relay(2)
    gather(4)
    move_all(0)
    sums(4)
    gather(5)
    relay(3)
    move_all(1)
    gather(6)
    sums(5)
    sums(6)
    gather(7)
    move_all(2)
    sums(7)
    for k in range(nz - 2, -1, -1):
        for q in late:
            for j in range(1, nx):
                leave(q, j, k)
            if k == 0:
                relay(q)
    for q in range(3, first):
        move_all(q)
    for k in range(nz - 1, 0, -1):
        for q in late:
            move_on(q, k)
        if k == nz - 1:
            settle(0)
            settle(1)
        elif k == nz - 2:
            for q in range(2, first):
                settle(q)
    for q in late:
        settle(q)

    for conds, copy in log:
        when(conds, lambda: copy().wait_send())
    pltpu.make_async_copy(out_v, out_ref, local_sem.at[2]).wait()
    each_own(lambda way: w_copy(None, y, way), finish)
    for step in range(1, ny):
        each_forward(lambda b, way: w_copy(None, b, way), step, finish, lambda b: None)
    side_all().wait_send()
    swap_copy(c).wait_send()
    aux_all().wait_send()
    count = (nx - 1) * nz * chunks
    if hyb:
        when([ends], lambda: x_total(count - chunks // 2).wait_send())
        when([inner], lambda: x_total(count - chunks).wait_send())
        when([ends], lambda: h_total(chunks // 2).wait_send())
        when([inner], lambda: h_total(chunks).wait_send())
    else:
        x_total(count).wait_send()
    for zz in range(nz):
        if zz < nz - 1:
            pl.when(z == zz)(lambda: z_total((nz - 1 - zz) * chunks, 1).wait_send())
        if zz > 0:
            pl.when(z == zz)(lambda: z_total(zz * chunks, 0).wait_send())


def body(
    nx,
    nc,
    tokens,
    norm_gain,
    expert_ids,
    route_weights,
    expert_gate,
    expert_up,
    expert_down,
    shared_gate,
    shared_up,
    shared_down,
    side_in,
    side_out,
    side_gate,
):
    tok_count, width = tokens.shape
    n_ep, n_tp = lax.axis_size("ep"), lax.axis_size("tp")
    nz, ny = n_ep // nx, n_tp // nc
    me = lax.axis_index("ep")
    local_experts, ff_part, _ = expert_gate.shape
    routed = local_experts * ff_part
    shared_rows = shared_gate.shape[0] // n_ep
    side_rows, side_all = side_in.shape
    side_cols = side_all // n_ep
    chunks = 8
    pieces = 2 * local_experts
    piece = width // chunks
    extra = -(-shared_rows // 16) * 16
    padded = -(-tok_count // 128) * 128

    def shared_part(array):
        if shared_rows % 16 == 0:
            return array
        own = lax.dynamic_slice_in_dim(array, me * shared_rows, shared_rows, 0)
        return jnp.pad(own, ((0, extra - shared_rows), (0, 0)))

    def side_part(array):
        if side_cols % 128 == 0:
            return array
        return array.reshape(side_rows, n_ep, side_cols).transpose(1, 0, 2)

    bf16, f32 = jnp.bfloat16, jnp.float32
    dma = pltpu.SemaphoreType.DMA
    dims = (nz, nx, ny, nc, local_experts, pieces, extra, chunks)
    return pl.pallas_call(
        functools.partial(kernel, dims),
        out_shape=jax.ShapeDtypeStruct((tok_count, width), bf16),
        in_specs=[pl.BlockSpec(memory_space=pl.ANY)]
        + [pl.BlockSpec(memory_space=pltpu.VMEM)] * 4
        + [pl.BlockSpec(memory_space=pl.ANY)] * 8,
        out_specs=pl.BlockSpec(memory_space=pl.ANY),
        scratch_shapes=[
            pltpu.VMEM((n_ep * tok_count, width), bf16),
            pltpu.VMEM((n_tp, 3 * (routed + extra), width), bf16),
            pltpu.VMEM((2 * n_ep, side_rows, side_cols), bf16),
            pltpu.VMEM((n_ep * tok_count, n_tp * (routed + extra)), bf16),
            pltpu.VMEM((n_ep * tok_count, side_cols), bf16),
            pltpu.VMEM((nz * chunks, tok_count, piece), f32),
            pltpu.VMEM(((nx - 1) * nz * chunks, tok_count, piece), bf16),
            pltpu.VMEM(((nx - 1) * nz * chunks, tok_count, piece), bf16),
            pltpu.VMEM((nz * chunks, tok_count, piece), bf16),
            pltpu.VMEM(((nz + 1) * chunks, tok_count, piece), bf16),
            pltpu.VMEM((chunks if nx == 2 else 1, tok_count, piece), bf16),
            pltpu.VMEM((n_ep, 8, padded), f32),
            pltpu.VMEM((n_ep, 8, padded), f32),
            pltpu.VMEM((n_ep * tok_count, 8), f32),
            pltpu.VMEM((tok_count, width), bf16),
            dma((nz, 1 + nx, 3)),
            dma((n_ep, 3)),
            dma((3,)),
            pltpu.SemaphoreType.REGULAR((nz,)),
            dma((ny, 1 + nc)),
            dma((pieces + chunks, n_tp)),
            dma,
            dma,
            dma,
            dma,
            dma((3,)),
            dma,
            dma,
            dma,
            dma(((nx - 1) * nz * chunks,)),
            dma,
            dma,
            dma(((nz + 1) * chunks,)),
            dma,
            dma((chunks,)),
        ],
        compiler_params=pltpu.CompilerParams(
            collective_id=0, has_side_effects=True, vmem_limit_bytes=63000 * 1024
        ),
        name="layer",
    )(
        tokens, norm_gain[None, :], expert_ids.T, route_weights.T, side_gate.reshape(-1, 128),
        expert_gate.reshape(routed, width), expert_up.reshape(routed, width),
        expert_down.reshape(routed, width), shared_part(shared_gate), shared_part(shared_up),
        shared_part(shared_down), side_part(side_in), side_part(side_out),
    )


def solution(mesh):
    devices = mesh.devices
    nx = len({d.coords[0] for d in devices[:, 0]})
    nc = len({d.core_on_chip for d in devices[0, :]})
    placed = (
        P(("ep", "tp"), None),
        P(),
        P(("ep", "tp"), None),
        P(("ep", "tp"), None),
        P("ep", "tp", None),
        P("ep", "tp", None),
        P("ep", "tp", None),
        P("tp", None),
        P("tp", None),
        P("tp", None),
        P("ep", None),
        P("ep", None),
        P(),
    )
    return jax.shard_map(
        functools.partial(body, nx, nc),
        mesh=mesh,
        in_specs=placed,
        out_specs=P(("ep", "tp"), None),
        check_vma=False,
    )
```

```python
import functools

import jax
import jax.numpy as jnp
from jax import lax
from jax.experimental import pallas as pl
from jax.experimental.pallas import tpu as pltpu
from jax.sharding import PartitionSpec as P

norm_eps = 1.0
MESH = pl.DeviceIdType.MESH
NT = (((1,), (1,)), ((), ()))


def silu(v):
    return v / (1.0 + jnp.exp(-v))


def when(conds, act):
    conds = [cond() for cond in conds]
    if any(cond is False for cond in conds):
        return
    conds = [cond for cond in conds if cond is not True]
    if not conds:
        act()
        return
    both = conds[0]
    for cond in conds[1:]:
        both = jnp.logical_and(both, cond)
    pl.when(both)(act)


def kernel(
    dims,
    tokens_ref, gain_ref, ids_ref, route_ref, side_gate_ref,
    gate_ref, up_ref, down_ref, s_gate_ref, s_up_ref, s_down_ref, side_in_ref, side_out_ref,
    out_ref,
    tok, wall, side, hidden, side_hid, acc, xs, xr, sent, got, hgot, saux, sc, scol, out_v,
    tok_send, tok_recv, hyb_send, know, w_send, w_recv, side_send, side_recv, swap_send, swap_recv,
    local_sem, aux_send, aux_recv, x_send, x_recv, r_send, l_send, z_recv, h_send, h_recv,
):
    nz, nx, ny, nc, local_experts, pieces, extra, chunks = dims
    n_ep, n_tp = nz * nx, ny * nc
    me, tp = lax.axis_index("ep"), lax.axis_index("tp")
    z, x = me // nx, me % nx
    y, c = tp // nc, tp % nc
    rows, width = tokens_ref.shape
    routed = gate_ref.shape[0]
    pr = routed // pieces
    per_expert = pieces // local_experts
    piece_units, shared_units = n_tp * pr, n_tp * extra
    side_rows, side_cols = side.shape[1:]
    piece = width // chunks
    unit_w = width // 16
    edges = [0, 5 * unit_w, 10 * unit_w, width]
    parts = len(edges) - 1
    down_at = 2 * (routed + extra)
    tile = 2 * rows
    hyb = nx == 2 and nz == 4
    tiles = n_ep // 2

    near = [
        sorted(range(nz), key=lambda b: (abs(b - zz), -b if 2 * zz < nz else b))
        for zz in range(nz)
    ]
    place_of = [[near[zz].index(b) for b in range(nz)] for zz in range(nz)]

    def by_z(values):
        out = values[0]
        if all(v == out for v in values):
            return out
        for zz in range(1, nz):
            out = jnp.where(z == zz, values[zz], out)
        return out

    def flag(values):
        values = [bool(v) for v in values]
        if all(values) or not any(values):
            return values[0]
        return by_z([int(v) for v in values]) == 1

    ends = lambda: flag([zz in (0, nz - 1) for zz in range(nz)])
    inner = lambda: flag([zz not in (0, nz - 1) for zz in range(nz)])
    twin = z + 1 - 2 * (z % 2)

    def slot(j, k):
        return k // 2 * (2 * nx) + 2 * j + k % 2

    def cols(q):
        return pl.ds(q * piece, piece)

    barrier = pltpu.get_barrier_semaphore()

    def tell(sem, ep, other):
        pl.semaphore_signal(sem, inc=1, device_id=(ep, other), device_id_type=MESH)

    def tell_near(sem):
        pl.when(z < nz - 1)(lambda: tell(sem, me + nx, tp))
        pl.when(z > 0)(lambda: tell(sem, me - nx, tp))
        for j in range(1, nx):
            tell(sem, z * nx + (x + j) % nx, tp)

    near_count = by_z([(zz > 0) + (zz < nz - 1) for zz in range(nz)]) + nx - 1
    tp_count = jnp.where(y > 0, 1, 0) + jnp.where(y < ny - 1, 1, 0) + nc - 1
    tell_near(barrier)
    pl.when(y < ny - 1)(lambda: tell(barrier, me, tp + nc))
    pl.when(y > 0)(lambda: tell(barrier, me, tp - nc))
    for j in range(1, nc):
        tell(barrier, me, y * nc + (c + j) % nc)
    load = pltpu.make_async_copy(tokens_ref, tok.at[pl.ds(0, tokens_ref.shape[0])], local_sem.at[2])
    load.start()


    def slot_rows(s):
        return pl.ds(s * rows if isinstance(s, int) else pl.multiple_of(s * rows, 16), rows)

    def tok_copy(from_slot, to_slot, h, target, send):
        part = pl.ds(edges[h], edges[h + 1] - edges[h])
        return pltpu.make_async_remote_copy(
            src_ref=tok.at[slot_rows(from_slot), part],
            dst_ref=tok.at[slot_rows(to_slot), part],
            send_sem=send, recv_sem=tok_recv.at[to_slot, h],
            device_id=target, device_id_type=MESH,
        )

    def tok_wait(s, h):
        tok_copy(s, s, h, (me, tp), tok_send.at[0, 0, 0]).wait_recv()

    def along(k, h, d):
        to = by_z([
            place_of[zz + d][near[zz][k]] if 0 <= zz + d < nz else 0 for zz in range(nz)
        ])
        return tok_copy(
            slot(0, k), slot(0, to), h, (me + d * nx, tp), tok_send.at[k, (1 - d) // 2, h]
        )

    def across(k, h, j):
        return tok_copy(
            slot(0, k), slot(nx - j, k), h, (z * nx + (x + j) % nx, tp), tok_send.at[k, 1 + j, h]
        )

    def onward(k, to, h):
        return tok_copy(
            slot(1, k), slot(1, to), h, (me + (twin - z) * nx, tp), hyb_send.at[h]
        )

    def crosses(k, h):
        if hyb and k == nz - 1 and h == parts - 1:
            return inner
        if hyb and k == nz - 2:
            return ends
        return lambda: True

    log = []

    def launch(conds, copy):
        log.append((conds, copy))
        when(conds, lambda: copy().start())

    def send_block(conds, k, h):
        bind = functools.partial
        for d in (1, -1):
            goes = [
                0 <= zz + d < nz and (near[zz][k] - zz) * d <= 0 for zz in range(nz)
            ]
            launch(conds + [lambda goes=goes: flag(goes)], bind(along, k, h, d))
        for j in range(1, nx):
            launch(conds + [crosses(k, h)], bind(across, k, h, j))

    def stage(step, h):
        for k in range(1, nz):
            here = [abs(near[zz][k] - zz) == step for zz in range(nz)]
            if any(here):
                cond = lambda here=here: flag(here)
                when([cond], lambda: tok_wait(slot(0, k), h))
                send_block([cond], k, h)
        if hyb and step == 1:
            tok_wait(slot(1, 0), h)
            launch([ends], functools.partial(onward, 0, nz - 2, h))
        if hyb and step == nz - 1 and h == parts - 1:
            when([inner], lambda: tok_wait(slot(1, nz - 1), h))
            launch([inner], functools.partial(onward, nz - 1, nz - 1, h))

    def cross_wait(half):
        for j in range(1, nx):
            for k in (2 * half, 2 * half + 1):
                for h in range(parts):
                    if hyb and k == 0:
                        continue
                    conds = [ends] if hyb and k == nz - 1 and h == parts - 1 else []
                    when(conds, lambda: tok_wait(slot(j, k), h))


    shared_at = pl.ds(0, extra)
    if s_gate_ref.shape[0] > extra:
        shared_at = pl.ds(pl.multiple_of(me * extra, extra), extra)

    def w_parts(k):
        slab = wall.at[tp]
        if k < pieces:
            at, r0 = pl.ds(k * pr, pr), 2 * extra + 2 * k * pr
            parts = [
                (gate_ref.at[at], slab.at[pl.ds(r0, pr)]),
                (up_ref.at[at], slab.at[pl.ds(r0 + pr, pr)]),
            ]
            if k == 0:
                parts += [
                    (s_gate_ref.at[shared_at], slab.at[pl.ds(0, extra)]),
                    (s_up_ref.at[shared_at], slab.at[pl.ds(extra, extra)]),
                ]
            return parts
        q = cols(k - pieces)
        return [
            (down_ref.at[:, q], slab.at[pl.ds(down_at, routed), q]),
            (s_down_ref.at[shared_at, q], slab.at[pl.ds(down_at + routed, extra), q]),
        ]

    def w_place(k, owner):
        if k == 0:
            return wall.at[owner, pl.ds(0, 2 * (extra + pr))]
        if k < pieces:
            return wall.at[owner, pl.ds(2 * (extra + k * pr), 2 * pr)]
        return wall.at[owner, pl.ds(down_at, routed + extra), cols(k - pieces)]

    def w_copy(k, by, way, refs=None):
        if way < 2:
            target = (me, tp + nc if way == 0 else tp - nc)
        else:
            target = (me, y * nc + (c + way - 1) % nc)
        owner = by * nc + c
        if refs is None:
            refs = (wall.at[owner],) * 2 if k is None else (w_place(k, owner),) * 2
        return pltpu.make_async_remote_copy(
            src_ref=refs[0], dst_ref=refs[1], send_sem=w_send.at[by, way],
            recv_sem=w_recv.at[0 if k is None else k, owner],
            device_id=target, device_id_type=MESH,
        )

    def w_wait(k, owner):
        pltpu.make_async_remote_copy(
            src_ref=w_place(k, owner), dst_ref=w_place(k, owner), send_sem=w_send.at[0, 0],
            recv_sem=w_recv.at[k, owner], device_id=(me, tp), device_id_type=MESH,
        ).wait_recv()

    def each_own(copy_of, act):
        pl.when(y < ny - 1)(lambda: act(copy_of(0)))
        pl.when(y > 0)(lambda: act(copy_of(1)))
        for way in range(2, 1 + nc):
            act(copy_of(way))

    def each_forward(copy_of, step, act, arrive):
        @pl.when(y >= step)
        def _():
            b = y - step
            arrive(b)
            pl.when(y < ny - 1)(lambda: act(copy_of(b, 0)))
            for way in range(2, 1 + nc):
                act(copy_of(b, way))

        @pl.when(y + step <= ny - 1)
        def _():
            b = y + step
            arrive(b)
            pl.when(y > 0)(lambda: act(copy_of(b, 1)))
            for way in range(2, 1 + nc):
                act(copy_of(b, way))

    start = lambda copy: copy.start()
    finish = lambda copy: copy.wait_send()

    def w_gathered(k):
        for step in range(1, ny):
            each_forward(
                lambda b, way: w_copy(k, b, way), step, start, lambda b: w_wait(k, b * nc + c)
            )

    def w_across(k):
        for j in range(1, nc):
            for by in range(ny):
                w_wait(k, by * nc + (c + j) % nc)


    def side_source(ref, to):
        if len(ref.shape) == 3:
            return ref.at[to]
        return ref.at[:, pl.ds(pl.multiple_of(to * side_cols, side_cols), side_cols)]

    def side_copy(j, p):
        to = (me + j) % n_ep
        return pltpu.make_async_remote_copy(
            src_ref=side_source((side_in_ref, side_out_ref)[p], to),
            dst_ref=side.at[p * n_ep + me],
            send_sem=side_send, recv_sem=side_recv, device_id=(to, tp), device_id_type=MESH,
        )

    def side_all():
        whole = side.at[pl.ds(0, n_ep - 1)]
        return pltpu.make_async_remote_copy(
            src_ref=whole, dst_ref=whole, send_sem=side_send, recv_sem=side_recv,
            device_id=(me, tp), device_id_type=MESH,
        )

    def side_own(p):
        return pltpu.make_async_copy(
            side_source((side_in_ref, side_out_ref)[p], me), side.at[p * n_ep + me],
            local_sem.at[1],
        )

    def swap_copy(half):
        part = side.at[pl.ds(half * n_ep, n_ep)]
        return pltpu.make_async_remote_copy(
            src_ref=part, dst_ref=part, send_sem=swap_send, recv_sem=swap_recv,
            device_id=(me, y * nc + 1 - c), device_id_type=MESH,
        )


    def aux_copy(k, j):
        to = by_z([near[zz][k] for zz in range(nz)]) * nx + (x + j) % nx
        k_there = by_z([place_of[near[zz][k]][zz] for zz in range(nz)])
        return pltpu.make_async_remote_copy(
            src_ref=saux.at[to], dst_ref=sc.at[slot((nx - j) % nx, k_there)],
            send_sem=aux_send, recv_sem=aux_recv, device_id=(to, tp), device_id_type=MESH,
        )

    def aux_all():
        return pltpu.make_async_remote_copy(
            src_ref=saux.at[pl.ds(0, n_ep - 1)], dst_ref=sc.at[pl.ds(0, n_ep - 1)],
            send_sem=aux_send, recv_sem=aux_recv, device_id=(me, tp), device_id_type=MESH,
        )

    for k in range(pieces + chunks):
        for part in w_parts(k):
            pltpu.make_async_copy(*part, local_sem.at[0]).start()
    for p in range(nc):
        pl.when(c == p)(lambda: side_own(p).start())

    pl.semaphore_wait(barrier, near_count + tp_count)
    for refs in w_parts(0):
        each_own(lambda way: w_copy(0, y, way, refs), start)
    load.wait()
    values = tok[slot_rows(0), :].astype(jnp.float32)
    scale_inv = lax.rsqrt(jnp.mean(values * values, axis=-1, keepdims=True) + norm_eps)
    normed = (values * scale_inv * gain_ref[...]).astype(jnp.bfloat16)
    tok[slot_rows(0), :] = normed

    for h in range(parts):
        send_block([], 0, h)
    tell_near(know.at[0])
    for k in range(1, pieces + chunks):
        for refs in w_parts(k):
            each_own(lambda way: w_copy(k, y, way, refs), start)

    for i in range(1, nz - 1):
        pl.semaphore_wait(know.at[i - 1], near_count)
        tell_near(know.at[i])
    side_vector = side_gate_ref[...].astype(jnp.float32)
    lanes = side_vector.shape[1]
    side_vector = jnp.concatenate(
        [jnp.broadcast_to(side_vector[i : i + 1], (8, lanes)) for i in range(width // lanes)],
        axis=1,
    ).astype(jnp.bfloat16)
    opening = lax.dot_general(side_vector, normed, NT, preferred_element_type=jnp.float32)
    opening = 1.0 / (1.0 + jnp.exp(-opening))
    ids, route = ids_ref[...], route_ref[...]
    row = lax.broadcasted_iota(jnp.int32, (8, rows), 0)
    for to in range(n_ep):
        block = jnp.where(row == local_experts, opening, 0.0)
        for e in range(local_experts):
            hit = jnp.where(ids == to * local_experts + e, route, 0.0)
            block = jnp.where(row == e, jnp.sum(hit, axis=0, keepdims=True), block)
        gap = sc.shape[2] - rows
        saux[to] = jnp.concatenate([block, jnp.zeros((8, gap), jnp.float32)], axis=1)
    sc[0] = saux[me]
    pl.semaphore_wait(know.at[nz - 2], near_count)
    for p in range(nc):
        def side_go(p=p):
            for j in range(1, n_ep):
                side_copy(j, p).start()

        pl.when(c == p)(side_go)
    for k in range(nz):
        for j in range(nx):
            if k or j:
                aux_copy(k, j).start()


    def tile_rows(t):
        return pl.ds(pl.multiple_of(t * tile, 16), tile)

    def column(at, n):
        picked = scol[at, :]
        lane = lax.broadcasted_iota(jnp.int32, picked.shape, 1)
        return jnp.sum(jnp.where(lane == n, picked, 0.0), axis=1, keepdims=True)

    def nt(a, b):
        return lax.dot_general(a, b, NT, preferred_element_type=jnp.float32)

    def unit(t, p):
        at = tile_rows(t)
        r0 = 2 * extra + p * (2 * pr)
        if not isinstance(p, int):
            r0 = pl.multiple_of(r0, 16)
        a = tok[at, :]
        gate = wall[:, pl.ds(r0, pr), :].reshape(piece_units, width)
        up = wall[:, pl.ds(r0 + pr, pr), :].reshape(piece_units, width)
        gated = silu(nt(a, gate)) * nt(a, up) * column(at, p // per_expert)
        to = p * piece_units if isinstance(p, int) else pl.multiple_of(p * piece_units, 128)
        hidden[at, pl.ds(to, piece_units)] = gated.astype(jnp.bfloat16)

    def units(t0, t1, p0, p1):
        n = p1 - p0
        if (t1 - t0) * n > 0:
            def step(i, carry):
                unit(t0 + i // n, p0 + i % n)
                return carry

            lax.fori_loop(0, (t1 - t0) * n, step, 0)

    def extras(t0, t1):
        def step(t, carry):
            at = tile_rows(t)
            a = tok[at, :]
            both = jnp.concatenate([
                wall[:, :extra, :].reshape(shared_units, width),
                wall[:, extra : 2 * extra, :].reshape(shared_units, width),
            ], axis=0)
            both = nt(a, both)
            gated = silu(both[:, :shared_units]) * both[:, shared_units:]
            hidden[at, pieces * piece_units :] = gated.astype(jnp.bfloat16)
            side_part = jnp.dot(
                a, side[:n_ep].reshape(width, side_cols), preferred_element_type=jnp.float32
            )
            side_hid[at] = (silu(side_part) * column(at, local_experts)).astype(jnp.bfloat16)
            return carry

        lax.fori_loop(t0, t1, step, 0)

    for h in range(parts):
        stage(1, h)
    pltpu.make_async_copy(wall.at[tp], wall.at[tp], local_sem.at[0]).wait()
    w_gathered(0)
    aux_all().wait_recv()
    for s in range(n_ep):
        scol[slot_rows(s), :] = sc[s].T[:rows]
    w_across(0)
    units(0, 1, 0, 1)
    for h in range(parts - 1):
        stage(2, h)
    w_gathered(1)
    stage(2, parts - 1)
    w_across(1)
    units(0, 1, 1, 2)
    cross_wait(0)
    units(1, nx, 0, 2)
    for s in range(3, nz):
        for h in range(parts - 1):
            stage(s, h)
    for p in range(2, pieces - 1):
        w_gathered(p)
    for p in range(nc):
        pl.when(c == p)(lambda: side_own(p).wait())
    side_all().wait_recv()
    swap_copy(c).start()
    for p in range(2, pieces - 1):
        w_across(p)
    units(0, nx, 2, pieces - 1)
    for s in range(3, nz):
        stage(s, parts - 1)
    units(nx, nx + 1, 0, pieces - 1)
    w_gathered(pieces - 1)
    swap_copy(1 - c).wait_recv()
    extras(0, nx + 1)
    w_across(pieces - 1)
    units(0, nx + 1, pieces - 1, pieces)
    w_gathered(pieces)
    for half in range(1, nz // 2):
        cross_wait(half)
    units(nx + 1, tiles, 0, pieces // 2)
    w_across(pieces)


    def x_index(j, k, q):
        return ((j - 1) * nz + k) * chunks + q

    def x_copy(q, j, k):
        i = x_index(j, k, q)
        return pltpu.make_async_remote_copy(
            src_ref=xs.at[i], dst_ref=xr.at[i], send_sem=x_send, recv_sem=x_recv.at[i],
            device_id=(z * nx + (x + j) % nx, tp), device_id_type=MESH,
        )

    def x_total(n):
        return pltpu.make_async_remote_copy(
            src_ref=xs.at[pl.ds(0, n)], dst_ref=xr.at[pl.ds(0, n)], send_sem=x_send,
            recv_sem=x_recv.at[0], device_id=(me, tp), device_id_type=MESH,
        )

    def h_copy(k, q):
        return pltpu.make_async_remote_copy(
            src_ref=xs.at[x_index(1, k, q)], dst_ref=hgot.at[q], send_sem=h_send,
            recv_sem=h_recv.at[q], device_id=(me + (twin - z) * nx, tp), device_id_type=MESH,
        )

    def h_total(n):
        return pltpu.make_async_remote_copy(
            src_ref=xs.at[pl.ds(0, n)], dst_ref=hgot.at[pl.ds(0, n)], send_sem=h_send,
            recv_sem=h_recv.at[0], device_id=(me, tp), device_id_type=MESH,
        )

    def z_copy(q, dz, right):
        return pltpu.make_async_remote_copy(
            src_ref=sent.at[dz * chunks + q], dst_ref=got.at[(dz + right) * chunks + q],
            send_sem=r_send if right else l_send, recv_sem=z_recv.at[(dz + right) * chunks + q],
            device_id=(me + nx if right else me - nx, tp), device_id_type=MESH,
        )

    def z_total(n, right):
        return pltpu.make_async_remote_copy(
            src_ref=sent.at[pl.ds(0, n)], dst_ref=got.at[pl.ds(0, n)],
            send_sem=r_send if right else l_send, recv_sem=z_recv.at[0],
            device_id=(me, tp), device_id_type=MESH,
        )

    blocks_per = piece // side_rows

    def product(q, j, half):
        down = jnp.concatenate(
            [
                wall[:, down_at + p * pr : down_at + (p + 1) * pr, cols(q)].reshape(
                    piece_units, piece
                )
                for p in range(pieces)
            ]
            + [wall[:, down_at + routed :, cols(q)].reshape(shared_units, piece)],
            axis=0,
        )
        side_down = side[pl.ds(n_ep + q * blocks_per, blocks_per)].reshape(piece, side_cols)
        at = tile_rows(half * nx + j)
        return jnp.dot(hidden[at], down, preferred_element_type=jnp.float32) + nt(
            side_hid[at], side_down
        )

    def detour(q, k):
        return hyb and k == 3 and q < chunks // 2

    def leave(q, j, k):
        go = lambda: x_copy(q, j, k).start()
        if detour(q, k):
            when([ends], lambda: h_copy(k, q).start())
        elif hyb and k == 2:
            when([ends], go)
        elif hyb and k == 0:
            when([inner], go)
        else:
            go()

    def partial_sum(q, half, j):
        value = product(q, j, half).astype(jnp.bfloat16)
        for i in (1, 0):
            k = 2 * half + i
            xs[x_index(j, k, q)] = value[i * rows : (i + 1) * rows]
            if q < chunks // 2 or k == nz - 1:
                leave(q, j, k)
            if hyb and k == 2:
                when([inner], lambda: h_copy(k, q).start())

    def own_sum(q, half):
        value = product(q, 0, half)
        for i in range(2):
            acc[(2 * half + i) * chunks + q] = value[i * rows : (i + 1) * rows]

    def relay(q):
        def pass_on(k):
            h_copy(k, q).wait_recv()
            i = x_index(1, k, q)
            value = xs[i].astype(jnp.float32) + hgot[q].astype(jnp.float32)
            xs[i] = value.astype(jnp.bfloat16)
            x_copy(q, 1, k).start()

        if hyb:
            when([ends], lambda: pass_on(0))
            if detour(q, 3):
                when([inner], lambda: pass_on(3))

    def fold(q, k):
        conds = []
        if detour(q, k):
            conds = [inner]
        if hyb and k == 2:
            conds = [ends]

        def add():
            value = acc[k * chunks + q]
            for j in range(1, nx):
                x_copy(q, j, k).wait_recv()
                value = value + xr[x_index(j, k, q)].astype(jnp.float32)
            acc[k * chunks + q] = value

        when(conds, add)

    def move_on(q, k):
        fold(q, k)
        dz = by_z([near[zz][k] for zz in range(nz)])

        def move(right, far):
            def act():
                value = acc[k * chunks + q]
                mine = dz * chunks + q

                @pl.when(z == far)
                def _():
                    sent[mine] = value.astype(jnp.bfloat16)

                @pl.when(z != far)
                def _():
                    z_copy(q, dz, right).wait_recv()
                    more = got[(dz + right) * chunks + q].astype(jnp.float32)
                    sent[mine] = (value + more).astype(jnp.bfloat16)

                z_copy(q, dz, right).start()

            return act

        when([lambda: flag([near[zz][k] > zz for zz in range(nz)])], move(1, 0))
        when([lambda: flag([near[zz][k] < zz for zz in range(nz)])], move(0, nz - 1))

    def settle(q):
        fold(q, 0)

        @pl.when(z > 0)
        def _():
            z_copy(q, z, 1).wait_recv()
            acc[q] += got[(z + 1) * chunks + q].astype(jnp.float32)

        @pl.when(z < nz - 1)
        def _():
            z_copy(q, z, 0).wait_recv()
            acc[q] += got[z * chunks + q].astype(jnp.float32)

        out_v[:, cols(q)] = acc[q].astype(jnp.bfloat16)
        pltpu.make_async_copy(out_v.at[:, cols(q)], out_ref.at[:, cols(q)], local_sem.at[2]).start()

    halves = nz // 2
    first = chunks // 2
    late = range(first, chunks)

    def own_sums(q):
        for half in reversed(range(halves)):
            own_sum(q, half)
            if half and detour(q, nz - 1):
                when([ends], lambda: move_on(q, nz - 1))

    def early(q):
        for j in range(1, nx):
            partial_sum(q, 0, j)
        own_sums(q)

    def rest(q):
        for half in reversed(range(1, halves)):
            for j in range(1, nx):
                partial_sum(q, half, j)

    def sums(q):
        w_across(pieces + q)
        rest(q)
        early(q)

    def move_all(q):
        if not detour(q, nz - 1):
            for k in range(nz - 1, 0, -1):
                move_on(q, k)
            return
        when([inner], lambda: move_on(q, 3))
        for k in (2, 1):
            when([ends], lambda: move_on(q, k))
            when([inner], lambda: move_on(q, 3 - k))

    gather = lambda q: w_gathered(pieces + q)
    early(0)
    gather(1)
    units(nx + 1, tiles, pieces // 2, pieces)
    w_across(pieces + 1)
    early(1)
    extras(nx + 1, tiles)
    gather(2)
    rest(0)
    rest(1)
    relay(0)
    gather(3)
    sums(2)
    relay(1)
    sums(3)
    relay(2)
    gather(4)
    move_all(0)
    sums(4)
    gather(5)
    relay(3)
    move_all(1)
    gather(6)
    sums(5)
    sums(6)
    gather(7)
    move_all(2)
    sums(7)
    for k in range(nz - 2, -1, -1):
        for q in late:
            for j in range(1, nx):
                leave(q, j, k)
            if k == 0:
                relay(q)
    for q in range(3, first):
        move_all(q)
    for k in range(nz - 1, 0, -1):
        for q in late:
            move_on(q, k)
        if k == nz - 1:
            settle(0)
            settle(1)
        elif k == nz - 2:
            for q in range(2, first):
                settle(q)
    for q in late:
        settle(q)

    for conds, copy in log:
        when(conds, lambda: copy().wait_send())
    pltpu.make_async_copy(out_v, out_ref, local_sem.at[2]).wait()
    each_own(lambda way: w_copy(None, y, way), finish)
    for step in range(1, ny):
        each_forward(lambda b, way: w_copy(None, b, way), step, finish, lambda b: None)
    side_all().wait_send()
    swap_copy(c).wait_send()
    aux_all().wait_send()
    count = (nx - 1) * nz * chunks
    if hyb:
        when([ends], lambda: x_total(count - chunks // 2).wait_send())
        when([inner], lambda: x_total(count - chunks).wait_send())
        when([ends], lambda: h_total(chunks // 2).wait_send())
        when([inner], lambda: h_total(chunks).wait_send())
    else:
        x_total(count).wait_send()
    for zz in range(nz):
        if zz < nz - 1:
            pl.when(z == zz)(lambda: z_total((nz - 1 - zz) * chunks, 1).wait_send())
        if zz > 0:
            pl.when(z == zz)(lambda: z_total(zz * chunks, 0).wait_send())


def body(
    nx,
    nc,
    tokens,
    norm_gain,
    expert_ids,
    route_weights,
    expert_gate,
    expert_up,
    expert_down,
    shared_gate,
    shared_up,
    shared_down,
    side_in,
    side_out,
    side_gate,
):
    tok_count, width = tokens.shape
    n_ep, n_tp = lax.axis_size("ep"), lax.axis_size("tp")
    nz, ny = n_ep // nx, n_tp // nc
    me = lax.axis_index("ep")
    local_experts, ff_part, _ = expert_gate.shape
    routed = local_experts * ff_part
    shared_rows = shared_gate.shape[0] // n_ep
    side_rows, side_all = side_in.shape
    side_cols = side_all // n_ep
    chunks = 8
    pieces = 2 * local_experts
    piece = width // chunks
    extra = -(-shared_rows // 16) * 16
    padded = -(-tok_count // 128) * 128

    def shared_part(array):
        if shared_rows % 16 == 0:
            return array
        own = lax.dynamic_slice_in_dim(array, me * shared_rows, shared_rows, 0)
        return jnp.pad(own, ((0, extra - shared_rows), (0, 0)))

    def side_part(array):
        if side_cols % 128 == 0:
            return array
        return array.reshape(side_rows, n_ep, side_cols).transpose(1, 0, 2)

    bf16, f32 = jnp.bfloat16, jnp.float32
    dma = pltpu.SemaphoreType.DMA
    dims = (nz, nx, ny, nc, local_experts, pieces, extra, chunks)
    return pl.pallas_call(
        functools.partial(kernel, dims),
        out_shape=jax.ShapeDtypeStruct((tok_count, width), bf16),
        in_specs=[pl.BlockSpec(memory_space=pl.ANY)]
        + [pl.BlockSpec(memory_space=pltpu.VMEM)] * 4
        + [pl.BlockSpec(memory_space=pl.ANY)] * 8,
        out_specs=pl.BlockSpec(memory_space=pl.ANY),
        scratch_shapes=[
            pltpu.VMEM((n_ep * tok_count, width), bf16),
            pltpu.VMEM((n_tp, 3 * (routed + extra), width), bf16),
            pltpu.VMEM((2 * n_ep, side_rows, side_cols), bf16),
            pltpu.VMEM((n_ep * tok_count, n_tp * (routed + extra)), bf16),
            pltpu.VMEM((n_ep * tok_count, side_cols), bf16),
            pltpu.VMEM((nz * chunks, tok_count, piece), f32),
            pltpu.VMEM(((nx - 1) * nz * chunks, tok_count, piece), bf16),
            pltpu.VMEM(((nx - 1) * nz * chunks, tok_count, piece), bf16),
            pltpu.VMEM((nz * chunks, tok_count, piece), bf16),
            pltpu.VMEM(((nz + 1) * chunks, tok_count, piece), bf16),
            pltpu.VMEM((chunks if nx == 2 else 1, tok_count, piece), bf16),
            pltpu.VMEM((n_ep, 8, padded), f32),
            pltpu.VMEM((n_ep, 8, padded), f32),
            pltpu.VMEM((n_ep * tok_count, 8), f32),
            pltpu.VMEM((tok_count, width), bf16),
            dma((nz, 1 + nx, 3)),
            dma((n_ep, 3)),
            dma((3,)),
            pltpu.SemaphoreType.REGULAR((nz,)),
            dma((ny, 1 + nc)),
            dma((pieces + chunks, n_tp)),
            dma,
            dma,
            dma,
            dma,
            dma((3,)),
            dma,
            dma,
            dma,
            dma(((nx - 1) * nz * chunks,)),
            dma,
            dma,
            dma(((nz + 1) * chunks,)),
            dma,
            dma((chunks,)),
        ],
        compiler_params=pltpu.CompilerParams(
            collective_id=0, has_side_effects=True, vmem_limit_bytes=63000 * 1024
        ),
        name="layer",
    )(
        tokens, norm_gain[None, :], expert_ids.T, route_weights.T, side_gate.reshape(-1, 128),
        expert_gate.reshape(routed, width), expert_up.reshape(routed, width),
        expert_down.reshape(routed, width), shared_part(shared_gate), shared_part(shared_up),
        shared_part(shared_down), side_part(side_in), side_part(side_out),
    )


def solution(mesh):
    devices = mesh.devices
    nx = len({d.coords[0] for d in devices[:, 0]})
    nc = len({d.core_on_chip for d in devices[0, :]})
    placed = (
        P(("ep", "tp"), None),
        P(),
        P(("ep", "tp"), None),
        P(("ep", "tp"), None),
        P("ep", "tp", None),
        P("ep", "tp", None),
        P("ep", "tp", None),
        P("tp", None),
        P("tp", None),
        P("tp", None),
        P("ep", None),
        P("ep", None),
        P(),
    )
    return jax.shard_map(
        functools.partial(body, nx, nc),
        mesh=mesh,
        in_specs=placed,
        out_specs=P(("ep", "tp"), None),
        check_vma=False,
    )
```
